512 devices in a mesh: gr: 2 (over z_hi), fs: 32 (over z_lo, y), tp: 8 (over x, core).
Axes of the slice: x: 4, y: 8, z: 8 (z_hi: 2, z_lo: 4; z = z_hi * 4 + z_lo), core: 2. Of those that a mesh axis runs over, the one named last changes fastest.
Arguments:
- prompt: bfloat16 [8192, 2048], P(('gr', 'fs')), may hold values from -6 to 6
- expert_ids: int32 [8192, 2], P(('gr', 'fs')), may hold values from 0 to 7, all different within a row; in each aligned block of 128 rows (0 to 127, 128 to 255, ...) at most 32 rows name the same one
- route_weights: float32 [8192, 2], P(('gr', 'fs')), may hold values from 0.2 to 1
- gate_master: float32 [8, 2048, 8192], P('gr', 'fs', 'tp'), may hold values from -0.125 to 0.125
- up_master: float32 [8, 2048, 8192], P('gr', 'fs', 'tp'), may hold values from -0.125 to 0.125
- down_master: float32 [8, 8192, 2048], P('gr', 'fs', 'tp'), may hold values from -0.0625 to 0.0625
- ffn_gain: float32 [2048], P('fs'), may hold values from 0.1 to 1.9
Outputs:
- gate_serving: bfloat16 [8, 2048, 8192], P('tp', None, 'fs')
- up_serving: bfloat16 [8, 2048, 8192], P('tp', None, 'fs')
- down_serving: bfloat16 [8, 8192, 2048], P('tp', 'fs')
- mixed: bfloat16 [8192, 2048], P(('gr', 'fs', 'tp'))
The draws below stay inside these ranges and needn't reach their ends.
Inputs may be any that keep to these rules, and one draw needn't show every extreme that they name: `expert_ids`: the two experts of a token differ; the rows of one index of gr and fs name each expert exactly 32 times.
All inputs are finite; a program needn't handle non-finite values.
Results may differ from the reference program's by a relative error of at most 0.025.
Values may be sent and summed in bfloat16 or wider, within the bound.
No kernel may reach another device: no remote copies, remote signals or barrier semaphores. Data moves between devices by JAX's collectives and lax.ppermute only.
A program may use at most 64 MiB of HBM per device.

```python
import math
import jax
import jax.numpy as jnp
import numpy as np
from jax import lax

D = 2048
FF = 8192
EXPERTS = 8
TOK_DEV = 128
SLOTS = 32
TOKENS = 8192
N_FS = 32


def block_scale(own_key, dims, cuts, low, largest):
    gain, own = 1.0, jax.random.fold_in(own_key, 6)
    for axis_at, parts in cuts:
        steps = jnp.exp(jax.random.uniform(jax.random.fold_in(own, axis_at), (parts,), jnp.float32, low / len(cuts), largest / len(cuts)))
        gain = gain * jnp.repeat(steps, dims[axis_at] // parts).reshape([-1 if axis == axis_at else 1 for axis in range(len(dims))])
    return gain


def deal_out(stream_key, own, number, rows, amount, top, reach, slope):
    sequence = jax.random.permutation(stream_key, amount)
    heavy_load, ordinary = load_shares(amount, rows * top, reach, slope, True), load_shares(amount, rows * top, reach, slope, False)
    places = jnp.arange(amount)

    def named(tallies, offset_by):
        used = int((tallies > 0).sum())
        fixed = max(1, used // 4)
        shifted = fixed + (places - fixed + offset_by * (used - fixed)) % max(1, amount - fixed)
        return jnp.zeros((amount,), jnp.int32).at[sequence[jnp.where(places < fixed, places, shifted)]].set(jnp.asarray(tallies, jnp.int32))

    tallies = jnp.where(number % 4 == 0, named(heavy_load, number // 4), named(ordinary, number - number // 4 - 1))
    mixed = jax.random.permutation(jax.random.fold_in(own, 3), amount)
    giver, sink = mixed[0:amount // 2 * 2:2], mixed[1:amount // 2 * 2:2]
    margin = jnp.minimum(tallies[giver] - 1, reach - tallies[sink]) // 2
    margin = jnp.where((giver == sequence[0]) | (sink == sequence[0]) | (tallies[sink] == 0), 0, jnp.maximum(margin, 0))
    shifted = jax.random.randint(jax.random.fold_in(own, 4), (amount // 2,), 0, 1 << 20) % (margin + 1)
    tallies = tallies.at[giver].add(-shifted).at[sink].add(shifted)
    items = jnp.searchsorted(jnp.cumsum(tallies), jnp.arange(rows * top), side="right").astype(jnp.int32)
    grid = items.reshape(top, rows).T
    grid = grid[jax.random.permutation(jax.random.fold_in(own, 1), rows)]
    offset_by = jax.random.randint(jax.random.fold_in(own, 2), (rows, 1), 0, top)
    return jnp.take_along_axis(grid, (jnp.arange(top)[None, :] + offset_by) % top, axis=1)


def load_shares(amount, total, bound, skew, full):
    portions = [(1 << 20) // math.isqrt(grade ** skew) + 1 for grade in range(1, amount + 1)]
    largest = bound if full else min(bound, max(-(-total // amount), total * portions[0] // sum(portions)))
    least = 1 if total - largest >= amount - 1 else 0
    holding, spare = [largest] + [least] * (amount - 1), total - largest - least * (amount - 1)
    while spare > 0:
        free = [i for i in range(1, amount) if holding[i] < largest] or [i for i in range(1, amount) if holding[i] < bound]
        whole, left = sum([portions[i] for i in free]), spare
        for i in free:
            more = min(bound - holding[i], max(1, left * portions[i] // whole), spare)
            holding[i] = holding[i] + more
            spare = spare - more
    return np.array(holding)


def gaussian(stream_key, extent, scale, limit, pieces=(), kind=jnp.bfloat16):
    factor_of = block_scale(stream_key, extent, pieces, -0.22, 0.18) if pieces else 1.0
    drawn = jax.random.normal(stream_key, extent, jnp.float32) * scale * factor_of
    return jnp.minimum(jnp.maximum(drawn, -limit), limit).astype(kind)


def setup_inputs(seed: int = 0) -> dict:
    keys = jax.random.split(jax.random.key(seed), 8)
    prompt = gaussian(keys[0], (TOKENS, D), 1.0, 6.0, ((0, 64),))
    expert_ids_keys = jax.random.split(jax.random.fold_in(keys[1], 1), TOKENS // TOK_DEV)
    expert_ids_turns = jax.random.permutation(jax.random.fold_in(keys[1], 3), TOKENS // TOK_DEV)
    expert_ids = jax.vmap(lambda own, number: deal_out(jax.random.fold_in(keys[1], 2), own, number, TOK_DEV, EXPERTS, 2, SLOTS, 0))(expert_ids_keys, expert_ids_turns).reshape((TOKENS, 2))
    route_weights = jnp.clip(0.2 + 0.8 * jax.random.uniform(keys[2], (TOKENS, 2), jnp.float32) ** block_scale(keys[2], (TOKENS, 2), ((0, 64),), -0.2, 0.2), 0.2, 1.0)
    gate_master = gaussian(keys[3], (EXPERTS, D, FF), D ** -0.5, 0.125, ((0, 2), (1, 32), (2, 8)), jnp.float32)
    up_master = gaussian(keys[4], (EXPERTS, D, FF), D ** -0.5, 0.125, ((0, 2), (1, 32), (2, 8)), jnp.float32)
    down_master = gaussian(keys[5], (EXPERTS, FF, D), FF ** -0.5, 0.0625, ((0, 2), (1, 32), (2, 8)), jnp.float32)
    ffn_gain = jnp.clip(1.0 + 0.18 * jax.random.normal(keys[6], (D,), jnp.float32), 0.1, 1.9)
    return dict(prompt=prompt, expert_ids=expert_ids, route_weights=route_weights, gate_master=gate_master, up_master=up_master, down_master=down_master, ffn_gain=ffn_gain)


NORM_EPS = 1e-06

def reference(prompt, expert_ids, route_weights, gate_master, up_master, down_master, ffn_gain):
    folding = ffn_gain[None, :, None]
    gate_serving = (gate_master * folding).astype(jnp.bfloat16)
    up_serving = (up_master * folding).astype(jnp.bfloat16)
    down_serving = down_master.astype(jnp.bfloat16)
    xfloat = prompt.astype(jnp.float32)
    normed = (xfloat * lax.rsqrt(lax.optimization_barrier(jnp.mean(xfloat * xfloat, axis=1, keepdims=True)) + NORM_EPS)).astype(jnp.bfloat16)
    pair_expert = expert_ids.reshape(-1)
    pair_weight = route_weights.reshape(-1)
    chosen = TOKENS * 2 // EXPERTS
    slice_width = FF // N_FS
    terms = jnp.zeros((TOKENS * 2, D), jnp.bfloat16)
    for expert in range(EXPERTS):
        ordering = jnp.argsort((pair_expert != expert).astype(jnp.int32), stable=True)[:chosen].astype(jnp.int32)
        rows_in = normed[ordering // 2]
        gate_part = jnp.dot(rows_in, gate_serving[expert], preferred_element_type=jnp.float32)
        up_part = jnp.dot(rows_in, up_serving[expert], preferred_element_type=jnp.float32)
        hidden = (jax.nn.silu(gate_part) * up_part).astype(jnp.bfloat16)
        down_one = down_serving[expert]

        def add_slice(total, index):
            start_row = (index * slice_width).astype(jnp.int32)
            hidden_block = lax.dynamic_slice_in_dim(hidden, start_row, slice_width, 1)
            weights = lax.dynamic_slice_in_dim(down_one, start_row, slice_width, 0)
            partial_sum = lax.optimization_barrier(jnp.dot(hidden_block, weights, preferred_element_type=jnp.float32).astype(jnp.bfloat16))
            return (total + partial_sum.astype(jnp.float32), None)
        expert_out, _ = lax.scan(add_slice, jnp.zeros((chosen, D), jnp.float32), jnp.arange(N_FS, dtype=jnp.int32))
        terms = terms.at[ordering].set((expert_out * pair_weight[ordering][:, None]).astype(jnp.bfloat16))
    mixed = lax.optimization_barrier(jnp.sum(terms.reshape(TOKENS, 2, D).astype(jnp.float32), axis=1)).astype(jnp.bfloat16)
    return (gate_serving, up_serving, down_serving, mixed)
```

```python
import jax
import jax.numpy as jnp
from jax import lax
from jax.experimental import pallas as pl
from jax.experimental.pallas import tpu as pltpu
from jax.sharding import Mesh
from jax.sharding import PartitionSpec as P

SLOTS = 32
NORM_EPS = 1e-06
FS = ("zl", "y")
TP = ("xh", "xl", "c")


def cut_kernel(gain_ref, w_ref, out_ref):
    width = out_ref.shape[-1]
    gain = gain_ref[...]
    for j in range(out_ref.shape[1]):
        out_ref[0, j, 0] = (w_ref[0, :, j * width : (j + 1) * width] * gain).astype(jnp.bfloat16)


def cut(master, gain):
    _, rows, width = master.shape
    cols = width // 4
    return pl.pallas_call(
        cut_kernel,
        grid=(4,),
        in_specs=[
            pl.BlockSpec((rows, 1), lambda e: (0, 0)),
            pl.BlockSpec((1, rows, width), lambda e: (e, 0, 0)),
        ],
        out_specs=pl.BlockSpec((1, 4, 1, rows, cols), lambda e: (e % 2, 0, e // 2, 0, 0)),
        out_shape=jax.ShapeDtypeStruct((2, 4, 2, rows, cols), jnp.bfloat16),
        name="cut",
    )(gain, master)


def slots_of(ids, expert):
    tokens = ids.shape[1]
    chosen = (ids[0:1] == expert) | (ids[1:2] == expert)
    before = lax.broadcasted_iota(jnp.int32, (tokens, tokens), 0) < lax.broadcasted_iota(
        jnp.int32, (tokens, tokens), 1
    )
    place = jnp.dot(
        chosen.astype(jnp.float32), before.astype(jnp.float32), preferred_element_type=jnp.float32
    ).astype(jnp.int32)
    slot = lax.broadcasted_iota(jnp.int32, (SLOTS, tokens), 0)
    return (place == slot) & chosen


def dispatch_kernel(expert_ref, ids_ref, prompt_ref, out_ref):
    x = prompt_ref[...].astype(jnp.float32)
    scale = lax.rsqrt(jnp.mean(x * x, axis=1, keepdims=True) + NORM_EPS)
    normed = (x * scale).astype(jnp.bfloat16)
    pick = slots_of(ids_ref[...], expert_ref[0]).astype(jnp.bfloat16)
    rows = jnp.dot(pick, normed, preferred_element_type=jnp.float32).astype(jnp.bfloat16)
    for z in range(out_ref.shape[0]):
        out_ref[z] = rows


def dispatch(expert, ids, prompt, copies):
    return pl.pallas_call(
        dispatch_kernel,
        in_specs=[
            pl.BlockSpec(memory_space=pltpu.SMEM),
            pl.BlockSpec(memory_space=pltpu.VMEM),
            pl.BlockSpec(memory_space=pltpu.VMEM),
        ],
        out_specs=pl.BlockSpec(memory_space=pltpu.VMEM),
        out_shape=jax.ShapeDtypeStruct((copies, SLOTS, prompt.shape[1]), jnp.bfloat16),
        name="dispatch",
    )(expert, ids, prompt)


def combine_kernel(expert_ref, ids_ref, weights_ref, parts_ref, out_ref):
    pick = slots_of(ids_ref[...], expert_ref[0])
    w = jnp.where(ids_ref[0:1] == expert_ref[0], weights_ref[0:1], weights_ref[1:2])
    slot_weight = jnp.sum(jnp.where(pick, w, 0.0), axis=1, keepdims=True)
    total = parts_ref[0].astype(jnp.float32)
    for z in range(1, parts_ref.shape[0]):
        total = total + parts_ref[z].astype(jnp.float32)
    term = (total * slot_weight).astype(jnp.bfloat16)
    out_ref[...] = lax.dot_general(
        pick.astype(jnp.bfloat16),
        term,
        (((0,), (0,)), ((), ())),
        preferred_element_type=jnp.float32,
    ).astype(jnp.bfloat16)


def combine(expert, ids, weights, parts):
    return pl.pallas_call(
        combine_kernel,
        in_specs=[
            pl.BlockSpec(memory_space=pltpu.SMEM),
            pl.BlockSpec(memory_space=pltpu.VMEM),
            pl.BlockSpec(memory_space=pltpu.VMEM),
            pl.BlockSpec(memory_space=pltpu.VMEM),
        ],
        out_specs=pl.BlockSpec(memory_space=pltpu.VMEM),
        out_shape=jax.ShapeDtypeStruct((ids.shape[1], parts.shape[2]), jnp.bfloat16),
        name="combine",
    )(expert, ids, weights, parts)


def place_kernel(at_ref, *refs):
    *pieces, out, sems = refs
    copies = []
    for k, piece in enumerate(pieces):
        copies.append(pltpu.make_async_copy(piece, out.at[k ^ at_ref[0]], sems.at[k]))
    for copy in copies:
        copy.start()
    for copy in copies:
        copy.wait()


def place(at, pieces):
    any_space = pl.BlockSpec(memory_space=pl.ANY)
    return pl.pallas_call(
        place_kernel,
        in_specs=[pl.BlockSpec(memory_space=pltpu.SMEM)] + [any_space] * len(pieces),
        out_specs=any_space,
        out_shape=jax.ShapeDtypeStruct((len(pieces), *pieces[0].shape), jnp.bfloat16),
        scratch_shapes=[pltpu.SemaphoreType.DMA((len(pieces),))],
        name="place",
    )(at, *pieces)


def place_cols_kernel(at_ref, *refs):
    *pieces, out, sems = refs
    copies = []
    for k, piece in enumerate(pieces):
        parts, _, width = piece.shape
        for i in range(parts):
            first = pl.multiple_of(((k ^ at_ref[0]) * parts + i) * width, width)
            copies.append(
                pltpu.make_async_copy(
                    piece.at[i], out.at[:, pl.ds(first, width)], sems.at[len(copies)]
                )
            )
    for copy in copies:
        copy.start()
    for copy in copies:
        copy.wait()


def place_cols(at, pieces):
    any_space = pl.BlockSpec(memory_space=pl.ANY)
    parts, rows, width = pieces[0].shape
    count = len(pieces) * parts
    return pl.pallas_call(
        place_cols_kernel,
        in_specs=[pl.BlockSpec(memory_space=pltpu.SMEM)] + [any_space] * len(pieces),
        out_specs=any_space,
        out_shape=jax.ShapeDtypeStruct((rows, count * width), jnp.bfloat16),
        scratch_shapes=[pltpu.SemaphoreType.DMA((count,))],
        name="place_cols",
    )(at, *pieces)


def exchange(value, axes):
    return lax.all_to_all(value, axes, split_axis=0, concat_axis=0, tiled=True)


def to_servers(blocks, zl, gr):
    _, _, _, rows, cols = blocks.shape
    by_core = exchange(blocks, "c")
    by_y = exchange(by_core.reshape(16, rows, cols), ("y", "xl")).reshape(8, 2, rows, cols)
    own = lax.dynamic_index_in_dim(by_y, zl & 1, 1, keepdims=False).reshape(8 * rows, cols)
    other = lax.dynamic_index_in_dim(by_y, 1 - (zl & 1), 1, keepdims=False).reshape(8 * rows, cols)
    pieces = []
    for k in range(4):
        pairs = []
        for g in range(2):
            for a in range(4):
                for p in range(2):
                    r, low = (k ^ a) >> 1, (k ^ a) & 1
                    pairs.append((g * 8 + a * 2 + p, r * 8 + (2 * p + low) * 2 + g))
        pieces.append(lax.ppermute(other if k & 1 else own, ("gr", "zl", "xh"), pairs))
    return place((2 * gr + (zl & 1)).reshape(1), pieces)


def down_to_servers(down, gr):
    by_tp = exchange(down, ("xl", "c"))
    pieces = []
    for k in range(2):
        pairs = [(g * 2 + p, (k ^ p) * 2 + g) for g in range(2) for p in range(2)]
        pieces.append(lax.ppermute(by_tp, ("gr", "xh"), pairs))
    return place_cols(gr.reshape(1), pieces)


def body(prompt, expert_ids, route_weights, gate_master, up_master, down_master, ffn_gain):
    gr, zl = lax.axis_index("gr"), lax.axis_index("zl")
    expert = lax.axis_index(TP).reshape(1)
    ids, weights = expert_ids.T, route_weights.T
    gain = ffn_gain[:, None]
    width = prompt.shape[1]

    gate = to_servers(cut(gate_master, gain), zl, gr)
    up = to_servers(cut(up_master, gain), zl, gr)
    down_serving = down_to_servers(down_master.astype(jnp.bfloat16), gr)
    gate_serving = gate.reshape(-1, gate.shape[-1])
    up_serving = up.reshape(-1, up.shape[-1])

    routed = exchange(dispatch(expert, ids, prompt, lax.axis_size("zl")), "zl")
    rows = lax.all_gather(routed, "y", axis=0, tiled=True).reshape(-1, width)
    gate_part = jnp.dot(rows, gate_serving, preferred_element_type=jnp.float32)
    up_part = jnp.dot(rows, up_serving, preferred_element_type=jnp.float32)
    hidden = (jax.nn.silu(gate_part) * up_part).astype(jnp.bfloat16)
    partial = jnp.dot(hidden, down_serving, preferred_element_type=jnp.float32).astype(jnp.bfloat16)
    partial = partial.reshape(-1, SLOTS, width)
    over_y = lax.psum_scatter(partial, "y", scatter_dimension=0, tiled=True)
    terms = combine(expert, ids, weights, exchange(over_y, "zl"))
    arrived = exchange(terms.reshape(lax.axis_size(TP), -1, width), TP)
    mixed = jnp.sum(arrived.astype(jnp.float32), axis=0).astype(jnp.bfloat16)
    return (gate_serving[None], up_serving[None], down_serving[None], mixed)


def solution(mesh):
    split = Mesh(
        mesh.devices.reshape(2, 4, 8, 2, 2, 2), ("gr", "zl", "y", "xh", "xl", "c")
    )
    placed = (
        P(("gr", *FS), None),
        P(("gr", *FS), None),
        P(("gr", *FS), None),
        P("gr", FS, TP),
        P("gr", FS, TP),
        P("gr", FS, TP),
        P(FS),
    )
    return jax.shard_map(
        body,
        mesh=split,
        in_specs=placed,
        out_specs=(P(TP, None, FS), P(TP, None, FS), P(TP, FS, None), P(("gr", *FS, *TP), None)),
        check_vma=False,
    )
```

```python
import jax
import jax.numpy as jnp
from jax import lax
from jax.experimental import pallas as pl
from jax.experimental.pallas import tpu as pltpu
from jax.sharding import Mesh
from jax.sharding import PartitionSpec as P

SLOTS = 32
NORM_EPS = 1e-06
FS = ("zl", "y")
TP = ("xh", "xl", "c")


def cut_kernel(gain_ref, gate_ref, up_ref, out_ref):
    width = out_ref.shape[-1]
    gain = gain_ref[...]
    for i, w_ref in enumerate((gate_ref, up_ref)):
        for j in range(out_ref.shape[2]):
            cols = w_ref[0, :, j * width : (j + 1) * width]
            out_ref[0, i, j, 0] = (cols * gain).astype(jnp.bfloat16)


def cut(gate, up, gain):
    _, rows, width = gate.shape
    cols = width // 4
    weights = pl.BlockSpec((1, rows, width), lambda e: (e, 0, 0))
    return pl.pallas_call(
        cut_kernel,
        grid=(4,),
        in_specs=[pl.BlockSpec((rows, 1), lambda e: (0, 0)), weights, weights],
        out_specs=pl.BlockSpec((1, 2, 4, 1, rows, cols), lambda e: (e % 2, 0, 0, e // 2, 0, 0)),
        out_shape=jax.ShapeDtypeStruct((2, 2, 4, 2, rows, cols), jnp.bfloat16),
        name="cut",
    )(gain, gate, up)


def slots_of(ids, expert):
    tokens = ids.shape[1]
    chosen = (ids[0:1] == expert) | (ids[1:2] == expert)
    before = lax.broadcasted_iota(jnp.int32, (tokens, tokens), 0) < lax.broadcasted_iota(
        jnp.int32, (tokens, tokens), 1
    )
    place = jnp.dot(
        chosen.astype(jnp.float32), before.astype(jnp.float32), preferred_element_type=jnp.float32
    ).astype(jnp.int32)
    slot = lax.broadcasted_iota(jnp.int32, (SLOTS, tokens), 0)
    return (place == slot) & chosen


def dispatch_kernel(expert_ref, ids_ref, prompt_ref, out_ref):
    x = prompt_ref[...].astype(jnp.float32)
    scale = lax.rsqrt(jnp.mean(x * x, axis=1, keepdims=True) + NORM_EPS)
    normed = (x * scale).astype(jnp.bfloat16)
    pick = slots_of(ids_ref[...], expert_ref[0]).astype(jnp.bfloat16)
    rows = jnp.dot(pick, normed, preferred_element_type=jnp.float32).astype(jnp.bfloat16)
    for z in range(out_ref.shape[0]):
        out_ref[z] = rows


def dispatch(expert, ids, prompt, copies):
    return pl.pallas_call(
        dispatch_kernel,
        in_specs=[
            pl.BlockSpec(memory_space=pltpu.SMEM),
            pl.BlockSpec(memory_space=pltpu.VMEM),
            pl.BlockSpec(memory_space=pltpu.VMEM),
        ],
        out_specs=pl.BlockSpec(memory_space=pltpu.VMEM),
        out_shape=jax.ShapeDtypeStruct((copies, SLOTS, prompt.shape[1]), jnp.bfloat16),
        name="dispatch",
    )(expert, ids, prompt)


def combine_kernel(expert_ref, ids_ref, weights_ref, parts_ref, out_ref):
    pick = slots_of(ids_ref[...], expert_ref[0])
    w = jnp.where(ids_ref[0:1] == expert_ref[0], weights_ref[0:1], weights_ref[1:2])
    slot_weight = jnp.sum(jnp.where(pick, w, 0.0), axis=1, keepdims=True)
    total = parts_ref[0].astype(jnp.float32)
    for z in range(1, parts_ref.shape[0]):
        total = total + parts_ref[z].astype(jnp.float32)
    term = (total * slot_weight).astype(jnp.bfloat16)
    out_ref[...] = lax.dot_general(
        pick.astype(jnp.bfloat16),
        term,
        (((0,), (0,)), ((), ())),
        preferred_element_type=jnp.float32,
    ).astype(jnp.bfloat16)


def combine(expert, ids, weights, parts):
    return pl.pallas_call(
        combine_kernel,
        in_specs=[
            pl.BlockSpec(memory_space=pltpu.SMEM),
            pl.BlockSpec(memory_space=pltpu.VMEM),
            pl.BlockSpec(memory_space=pltpu.VMEM),
            pl.BlockSpec(memory_space=pltpu.VMEM),
        ],
        out_specs=pl.BlockSpec(memory_space=pltpu.VMEM),
        out_shape=jax.ShapeDtypeStruct((ids.shape[1], parts.shape[2]), jnp.bfloat16),
        name="combine",
    )(expert, ids, weights, parts)


def place_kernel(at_ref, *refs):
    *pieces, out_ref = refs
    for k, piece in enumerate(pieces):
        out_ref[k ^ at_ref[0]] = piece[...]


def place(at, pieces):
    return pl.pallas_call(
        place_kernel,
        in_specs=[pl.BlockSpec(memory_space=pltpu.SMEM)]
        + [pl.BlockSpec(memory_space=pltpu.VMEM)] * len(pieces),
        out_specs=pl.BlockSpec(memory_space=pltpu.VMEM),
        out_shape=jax.ShapeDtypeStruct((len(pieces), *pieces[0].shape), jnp.bfloat16),
        name="place",
    )(at, *pieces)


def place_cols_kernel(at_ref, blocks_ref, out_ref):
    out_ref[...] = blocks_ref[0, 0]


def place_cols(at, blocks):
    parts, pieces, rows, width = blocks.shape
    return pl.pallas_call(
        place_cols_kernel,
        grid_spec=pltpu.PrefetchScalarGridSpec(
            num_scalar_prefetch=1,
            grid=(pieces, parts),
            in_specs=[pl.BlockSpec((1, 1, rows, width), lambda k, i, at: (i, k, 0, 0))],
            out_specs=pl.BlockSpec((rows, width), lambda k, i, at: (0, (k ^ at[0]) * parts + i)),
        ),
        out_shape=jax.ShapeDtypeStruct((rows, pieces * parts * width), jnp.bfloat16),
        name="place_cols",
    )(at, blocks)


def exchange(value, axes):
    return lax.all_to_all(value, axes, split_axis=0, concat_axis=0, tiled=True)


def to_servers(by_core, zl, gr):
    _, _, _, rows, cols = by_core.shape
    by_y = exchange(by_core.reshape(16, rows, cols), ("y", "xl")).reshape(8, 2, rows, cols)
    own = lax.dynamic_index_in_dim(by_y, zl & 1, 1, keepdims=False).reshape(8 * rows, cols)
    other = lax.dynamic_index_in_dim(by_y, 1 - (zl & 1), 1, keepdims=False).reshape(8 * rows, cols)
    pieces = []
    for k in range(4):
        pairs = []
        for g in range(2):
            for a in range(4):
                for p in range(2):
                    r, low = (k ^ a) >> 1, (k ^ a) & 1
                    pairs.append((g * 8 + a * 2 + p, r * 8 + (2 * p + low) * 2 + g))
        pieces.append(lax.ppermute(other if k & 1 else own, ("gr", "zl", "xh"), pairs))
    return place((2 * gr + (zl & 1)).reshape(1), pieces)


def down_to_servers(down, gr):
    pieces = []
    for k in range(2):
        pairs = [(g * 2 + p, (k ^ p) * 2 + g) for g in range(2) for p in range(2)]
        pieces.append(lax.ppermute(down, ("gr", "xh"), pairs))
    return place_cols(gr.reshape(1), exchange(jnp.stack(pieces, axis=1), ("xl", "c")))


def body(prompt, expert_ids, route_weights, gate_master, up_master, down_master, ffn_gain):
    gr, zl = lax.axis_index("gr"), lax.axis_index("zl")
    expert = lax.axis_index(TP).reshape(1)
    ids, weights = expert_ids.T, route_weights.T
    gain = ffn_gain[:, None]
    width = prompt.shape[1]

    down_serving = down_to_servers(down_master.astype(jnp.bfloat16), gr)
    by_core = exchange(cut(gate_master, up_master, gain), "c")
    prompt, by_core = lax.optimization_barrier((prompt, by_core))
    gate = to_servers(by_core[:, 0], zl, gr)
    up = to_servers(by_core[:, 1], zl, gr)
    gate_serving = gate.reshape(-1, gate.shape[-1])
    up_serving = up.reshape(-1, up.shape[-1])

    routed = exchange(dispatch(expert, ids, prompt, lax.axis_size("zl")), "zl")
    rows = lax.all_gather(routed, "y", axis=0, tiled=True).reshape(-1, width)
    gate_part = jnp.dot(rows, gate_serving, preferred_element_type=jnp.float32)
    up_part = jnp.dot(rows, up_serving, preferred_element_type=jnp.float32)
    hidden = (jax.nn.silu(gate_part) * up_part).astype(jnp.bfloat16)
    partial = jnp.dot(hidden, down_serving, preferred_element_type=jnp.float32).astype(jnp.bfloat16)
    partial = partial.reshape(-1, SLOTS, width)
    over_y = lax.psum_scatter(partial, "y", scatter_dimension=0, tiled=True)
    terms = combine(expert, ids, weights, exchange(over_y, "zl"))
    arrived = exchange(terms.reshape(lax.axis_size(TP), -1, width), TP)
    mixed = jnp.sum(arrived.astype(jnp.float32), axis=0).astype(jnp.bfloat16)
    return (gate_serving[None], up_serving[None], down_serving[None], mixed)


def solution(mesh):
    split = Mesh(
        mesh.devices.reshape(2, 4, 8, 2, 2, 2), ("gr", "zl", "y", "xh", "xl", "c")
    )
    placed = (
        P(("gr", *FS), None),
        P(("gr", *FS), None),
        P(("gr", *FS), None),
        P("gr", FS, TP),
        P("gr", FS, TP),
        P("gr", FS, TP),
        P(FS),
    )
    return jax.shard_map(
        body,
        mesh=split,
        in_specs=placed,
        out_specs=(P(TP, None, FS), P(TP, None, FS), P(TP, FS, None), P(("gr", *FS, *TP), None)),
        check_vma=False,
    )
```

```python
import jax
import jax.numpy as jnp
from jax import lax
from jax.experimental import pallas as pl
from jax.experimental.pallas import tpu as pltpu
from jax.sharding import Mesh
from jax.sharding import PartitionSpec as P


SLOTS = 32
NORM_EPS = 1e-06
FS = ("zl", "y")
TP = ("xh", "xl", "c")


def cut_kernel(gain_ref, gate_ref, up_ref, out_ref):
    width = out_ref.shape[-1]
    gain = gain_ref[...]
    for i, w_ref in enumerate((gate_ref, up_ref)):
        for j in range(out_ref.shape[2]):
            cols = w_ref[0, :, j * width : (j + 1) * width]
            out_ref[0, i, j, 0] = (cols * gain).astype(jnp.bfloat16)


def cut(gate, up, gain):
    _, rows, width = gate.shape
    cols = width // 4
    weights = pl.BlockSpec((1, rows, width), lambda e: (e, 0, 0))
    return pl.pallas_call(
        cut_kernel,
        grid=(4,),
        in_specs=[pl.BlockSpec((rows, 1), lambda e: (0, 0)), weights, weights],
        out_specs=pl.BlockSpec((1, 2, 4, 1, rows, cols), lambda e: (e % 2, 0, 0, e // 2, 0, 0)),
        out_shape=jax.ShapeDtypeStruct((2, 2, 4, 2, rows, cols), jnp.bfloat16),
        name="cut",
    )(gain, gate, up)


def slots_of(ids, expert):
    tokens = ids.shape[1]
    chosen = (ids[0:1] == expert) | (ids[1:2] == expert)
    before = lax.broadcasted_iota(jnp.int32, (tokens, tokens), 0) < lax.broadcasted_iota(
        jnp.int32, (tokens, tokens), 1
    )
    place = jnp.dot(
        chosen.astype(jnp.float32), before.astype(jnp.float32), preferred_element_type=jnp.float32
    ).astype(jnp.int32)
    slot = lax.broadcasted_iota(jnp.int32, (SLOTS, tokens), 0)
    return (place == slot) & chosen


def dispatch_kernel(expert_ref, ids_ref, prompt_ref, out_ref):
    x = prompt_ref[...].astype(jnp.float32)
    scale = lax.rsqrt(jnp.mean(x * x, axis=1, keepdims=True) + NORM_EPS)
    normed = (x * scale).astype(jnp.bfloat16)
    pick = slots_of(ids_ref[...], expert_ref[0]).astype(jnp.bfloat16)
    rows = jnp.dot(pick, normed, preferred_element_type=jnp.float32).astype(jnp.bfloat16)
    for z in range(out_ref.shape[0]):
        out_ref[z] = rows


def dispatch(expert, ids, prompt, copies):
    return pl.pallas_call(
        dispatch_kernel,
        in_specs=[
            pl.BlockSpec(memory_space=pltpu.SMEM),
            pl.BlockSpec(memory_space=pltpu.VMEM),
            pl.BlockSpec(memory_space=pltpu.VMEM),
        ],
        out_specs=pl.BlockSpec(memory_space=pltpu.VMEM),
        out_shape=jax.ShapeDtypeStruct((copies, SLOTS, prompt.shape[1]), jnp.bfloat16),
        name="dispatch",
    )(expert, ids, prompt)


def combine_kernel(expert_ref, ids_ref, weights_ref, parts_ref, out_ref):
    pick = slots_of(ids_ref[...], expert_ref[0])
    w = jnp.where(ids_ref[0:1] == expert_ref[0], weights_ref[0:1], weights_ref[1:2])
    slot_weight = jnp.sum(jnp.where(pick, w, 0.0), axis=1, keepdims=True)
    total = parts_ref[0].astype(jnp.float32)
    for z in range(1, parts_ref.shape[0]):
        total = total + parts_ref[z].astype(jnp.float32)
    term = (total * slot_weight).astype(jnp.bfloat16)
    out_ref[...] = lax.dot_general(
        pick.astype(jnp.bfloat16),
        term,
        (((0,), (0,)), ((), ())),
        preferred_element_type=jnp.float32,
    ).astype(jnp.bfloat16)


def combine(expert, ids, weights, parts):
    return pl.pallas_call(
        combine_kernel,
        in_specs=[
            pl.BlockSpec(memory_space=pltpu.SMEM),
            pl.BlockSpec(memory_space=pltpu.VMEM),
            pl.BlockSpec(memory_space=pltpu.VMEM),
            pl.BlockSpec(memory_space=pltpu.VMEM),
        ],
        out_specs=pl.BlockSpec(memory_space=pltpu.VMEM),
        out_shape=jax.ShapeDtypeStruct((ids.shape[1], parts.shape[2]), jnp.bfloat16),
        name="combine",
    )(expert, ids, weights, parts)


def place_kernel(at_ref, *refs):
    *pieces, out_ref = refs
    for k, piece in enumerate(pieces):
        out_ref[k ^ at_ref[0]] = piece[...]


def place(at, pieces):
    return pl.pallas_call(
        place_kernel,
        in_specs=[pl.BlockSpec(memory_space=pltpu.SMEM)]
        + [pl.BlockSpec(memory_space=pltpu.VMEM)] * len(pieces),
        out_specs=pl.BlockSpec(memory_space=pltpu.VMEM),
        out_shape=jax.ShapeDtypeStruct((len(pieces), *pieces[0].shape), jnp.bfloat16),
        name="place",
    )(at, *pieces)


def place_cols_kernel(at_ref, blocks_ref, out_ref):
    out_ref[...] = blocks_ref[0, 0]


def place_cols(at, blocks):
    parts, pieces, rows, width = blocks.shape
    return pl.pallas_call(
        place_cols_kernel,
        grid_spec=pltpu.PrefetchScalarGridSpec(
            num_scalar_prefetch=1,
            grid=(pieces, parts),
            in_specs=[pl.BlockSpec((1, 1, rows, width), lambda k, i, at: (i, k, 0, 0))],
            out_specs=pl.BlockSpec((rows, width), lambda k, i, at: (0, (k ^ at[0]) * parts + i)),
        ),
        out_shape=jax.ShapeDtypeStruct((rows, pieces * parts * width), jnp.bfloat16),
        name="place_cols",
    )(at, blocks)


def exchange(value, axes):
    return lax.all_to_all(value, axes, split_axis=0, concat_axis=0, tiled=True)


def by_half(by_core, zl):
    _, _, _, rows, cols = by_core.shape
    by_y = exchange(by_core.reshape(16, rows, cols), ("y", "xl"))
    by_y = by_y.reshape(8, 2, rows, cols)
    own = lax.dynamic_index_in_dim(by_y, zl & 1, 1, keepdims=False).reshape(8 * rows, cols)
    other = lax.dynamic_index_in_dim(by_y, 1 - (zl & 1), 1, keepdims=False).reshape(8 * rows, cols)
    return own, other


def to_servers(own, other, zl, gr):
    pieces = []
    for k in range(4):
        pairs = []
        for g in range(2):
            for a in range(4):
                for p in range(2):
                    r, low = (k ^ a) >> 1, (k ^ a) & 1
                    pairs.append((g * 8 + a * 2 + p, r * 8 + (2 * p + low) * 2 + g))
        pieces.append(lax.ppermute(other if k & 1 else own, ("gr", "zl", "xh"), pairs))
    return place((2 * gr + (zl & 1)).reshape(1), pieces)


def down_to_servers(down, gr):
    pieces = []
    for k in range(2):
        pairs = [(g * 2 + p, (k ^ p) * 2 + g) for g in range(2) for p in range(2)]
        pieces.append(lax.ppermute(down, ("gr", "xh"), pairs))
    blocks = jnp.stack(pieces, axis=1)
    return place_cols(gr.reshape(1), exchange(blocks, ("xl", "c")))


def body(prompt, expert_ids, route_weights, gate_master, up_master, down_master, ffn_gain):
    gr, zl = lax.axis_index("gr"), lax.axis_index("zl")
    expert = lax.axis_index(TP).reshape(1)
    ids, weights = expert_ids.T, route_weights.T
    gain = ffn_gain[:, None]
    width = prompt.shape[1]

    routed = exchange(dispatch(expert, ids, prompt, lax.axis_size("zl")), "zl")
    down_serving = down_to_servers(down_master.astype(jnp.bfloat16), gr)
    blocks = cut(gate_master, up_master, gain)
    by_core = exchange(blocks, "c")
    own, other = by_half(by_core[:, 0], zl)
    own, other, up_blocks = lax.optimization_barrier((own, other, by_core[:, 1]))
    gate = to_servers(own, other, zl, gr)
    up = to_servers(*by_half(up_blocks, zl), zl, gr)
    gate_serving = gate.reshape(-1, gate.shape[-1])
    up_serving = up.reshape(-1, up.shape[-1])

    rows = lax.all_gather(routed, "y", axis=0, tiled=True).reshape(-1, width)
    gate_part = jnp.dot(rows, gate_serving, preferred_element_type=jnp.float32)
    up_part = jnp.dot(rows, up_serving, preferred_element_type=jnp.float32)
    hidden = (jax.nn.silu(gate_part) * up_part).astype(jnp.bfloat16)
    partial = jnp.dot(hidden, down_serving, preferred_element_type=jnp.float32).astype(jnp.bfloat16)
    partial = partial.reshape(-1, SLOTS, width)
    over_y = lax.psum_scatter(partial, "y", scatter_dimension=0, tiled=True)
    terms = combine(expert, ids, weights, exchange(over_y, "zl"))
    arrived = exchange(terms.reshape(lax.axis_size(TP), -1, width), TP)
    mixed = jnp.sum(arrived.astype(jnp.float32), axis=0).astype(jnp.bfloat16)
    return (gate_serving[None], up_serving[None], down_serving[None], mixed)


def solution(mesh):
    split = Mesh(
        mesh.devices.reshape(2, 4, 8, 2, 2, 2), ("gr", "zl", "y", "xh", "xl", "c")
    )
    placed = (
        P(("gr", *FS), None),
        P(("gr", *FS), None),
        P(("gr", *FS), None),
        P("gr", FS, TP),
        P("gr", FS, TP),
        P("gr", FS, TP),
        P(FS),
    )
    return jax.shard_map(
        body,
        mesh=split,
        in_specs=placed,
        out_specs=(P(TP, None, FS), P(TP, None, FS), P(TP, FS, None), P(("gr", *FS, *TP), None)),
        check_vma=False,
    )
```

```python
import jax
import jax.numpy as jnp
from jax import lax
from jax.experimental import pallas as pl
from jax.experimental.pallas import tpu as pltpu
from jax.sharding import Mesh
from jax.sharding import PartitionSpec as P


SLOTS = 32
NEAR = 1408
NORM_EPS = 1e-06
FS = ("zl", "y")
TP = ("xh", "xl", "c")


def cut_kernel(gain_ref, gate_ref, up_ref, out_ref):
    width = out_ref.shape[-1]
    gain = gain_ref[...]
    for i, w_ref in enumerate((gate_ref, up_ref)):
        for j in range(out_ref.shape[2]):
            cols = w_ref[0, :, j * width : (j + 1) * width]
            out_ref[0, i, j, 0] = (cols * gain).astype(jnp.bfloat16)


def cut(gate, up, gain):
    _, rows, width = gate.shape
    cols = width // 4
    weights = pl.BlockSpec((1, rows, width), lambda e: (e, 0, 0))
    return pl.pallas_call(
        cut_kernel,
        grid=(4,),
        in_specs=[pl.BlockSpec((rows, 1), lambda e: (0, 0)), weights, weights],
        out_specs=pl.BlockSpec((1, 2, 4, 1, rows, cols), lambda e: (e % 2, 0, 0, e // 2, 0, 0)),
        out_shape=jax.ShapeDtypeStruct((2, 2, 4, 2, rows, cols), jnp.bfloat16),
        name="cut",
    )(gain, gate, up)


def slots_of(ids, expert):
    tokens = ids.shape[1]
    chosen = (ids[0:1] == expert) | (ids[1:2] == expert)
    before = lax.broadcasted_iota(jnp.int32, (tokens, tokens), 0) < lax.broadcasted_iota(
        jnp.int32, (tokens, tokens), 1
    )
    place = jnp.dot(
        chosen.astype(jnp.float32), before.astype(jnp.float32), preferred_element_type=jnp.float32
    ).astype(jnp.int32)
    slot = lax.broadcasted_iota(jnp.int32, (SLOTS, tokens), 0)
    return (place == slot) & chosen


def dispatch_kernel(expert_ref, ids_ref, prompt_ref, out_ref):
    x = prompt_ref[...].astype(jnp.float32)
    scale = lax.rsqrt(jnp.mean(x * x, axis=1, keepdims=True) + NORM_EPS)
    normed = (x * scale).astype(jnp.bfloat16)
    pick = slots_of(ids_ref[...], expert_ref[0]).astype(jnp.bfloat16)
    out_ref[...] = jnp.dot(pick, normed, preferred_element_type=jnp.float32).astype(jnp.bfloat16)


def dispatch(expert, ids, prompt):
    return pl.pallas_call(
        dispatch_kernel,
        in_specs=[
            pl.BlockSpec(memory_space=pltpu.SMEM),
            pl.BlockSpec(memory_space=pltpu.VMEM),
            pl.BlockSpec(memory_space=pltpu.VMEM),
        ],
        out_specs=pl.BlockSpec(memory_space=pltpu.VMEM),
        out_shape=jax.ShapeDtypeStruct((SLOTS, prompt.shape[1]), jnp.bfloat16),
        name="dispatch",
    )(expert, ids, prompt)


def summed(parts):
    total = parts[0].astype(jnp.float32)
    for part in parts[1:]:
        total = total + part.astype(jnp.float32)
    return total


def combine_kernel(expert_ref, ids_ref, weights_ref, far_ref, *refs):
    *near_refs, out_ref = refs
    pick = slots_of(ids_ref[...], expert_ref[0])
    w = jnp.where(ids_ref[0:1] == expert_ref[0], weights_ref[0:1], weights_ref[1:2])
    slot_weight = jnp.sum(jnp.where(pick, w, 0.0), axis=1, keepdims=True)
    pick = pick.astype(jnp.bfloat16)
    split = near_refs[0].shape[1]
    totals = (
        (0, summed([ref[...] for ref in near_refs])),
        (split, summed([far_ref[i] for i in range(far_ref.shape[0])])),
    )
    for first, total in totals:
        out_ref[:, first : first + total.shape[1]] = lax.dot_general(
            pick,
            (total * slot_weight).astype(jnp.bfloat16),
            (((0,), (0,)), ((), ())),
            preferred_element_type=jnp.float32,
        ).astype(jnp.bfloat16)


def combine(expert, ids, weights, near, far):
    vmem = pl.BlockSpec(memory_space=pltpu.VMEM)
    width = near[0].shape[1] + far.shape[2]
    return pl.pallas_call(
        combine_kernel,
        in_specs=[pl.BlockSpec(memory_space=pltpu.SMEM)] + [vmem] * (3 + len(near)),
        out_specs=vmem,
        out_shape=jax.ShapeDtypeStruct((ids.shape[1], width), jnp.bfloat16),
        name="combine",
    )(expert, ids, weights, far, *near)


def place_kernel(at_ref, *refs):
    *pieces, out_ref = refs
    for k, piece in enumerate(pieces):
        out_ref[k ^ at_ref[0]] = piece[...]


def place(at, pieces):
    return pl.pallas_call(
        place_kernel,
        in_specs=[pl.BlockSpec(memory_space=pltpu.SMEM)]
        + [pl.BlockSpec(memory_space=pltpu.VMEM)] * len(pieces),
        out_specs=pl.BlockSpec(memory_space=pltpu.VMEM),
        out_shape=jax.ShapeDtypeStruct((len(pieces), *pieces[0].shape), jnp.bfloat16),
        name="place",
    )(at, *pieces)


def place_cols_kernel(at_ref, blocks_ref, out_ref):
    out_ref[...] = blocks_ref[0, 0]


def place_cols(at, blocks):
    parts, pieces, rows, width = blocks.shape
    return pl.pallas_call(
        place_cols_kernel,
        grid_spec=pltpu.PrefetchScalarGridSpec(
            num_scalar_prefetch=1,
            grid=(pieces, parts),
            in_specs=[pl.BlockSpec((1, 1, rows, width), lambda k, i, at: (i, k, 0, 0))],
            out_specs=pl.BlockSpec((rows, width), lambda k, i, at: (0, (k ^ at[0]) * parts + i)),
        ),
        out_shape=jax.ShapeDtypeStruct((rows, pieces * parts * width), jnp.bfloat16),
        name="place_cols",
    )(at, blocks)


def exchange(value, axes):
    return lax.all_to_all(value, axes, split_axis=0, concat_axis=0, tiled=True)


def shifted(value, step):
    count = lax.axis_size("zl")
    pairs = [(z, (z + step) % count) for z in range(count)]
    return lax.ppermute(value, "zl", pairs)


def by_half(by_core, zl):
    _, _, _, rows, cols = by_core.shape
    by_y = exchange(by_core.reshape(16, rows, cols), ("y", "xl"))
    by_y = by_y.reshape(8, 2, rows, cols)
    own = lax.dynamic_index_in_dim(by_y, zl & 1, 1, keepdims=False).reshape(8 * rows, cols)
    other = lax.dynamic_index_in_dim(by_y, 1 - (zl & 1), 1, keepdims=False).reshape(8 * rows, cols)
    return own, other


def to_servers(own, other, zl, gr):
    pieces = []
    for k in range(4):
        pairs = []
        for g in range(2):
            for a in range(4):
                for p in range(2):
                    r, low = (k ^ a) >> 1, (k ^ a) & 1
                    pairs.append((g * 8 + a * 2 + p, r * 8 + (2 * p + low) * 2 + g))
        pieces.append(lax.ppermute(other if k & 1 else own, ("gr", "zl", "xh"), pairs))
    return place((2 * gr + (zl & 1)).reshape(1), pieces)


def down_to_servers(down, gr):
    pieces = []
    for k in range(2):
        pairs = [(g * 2 + p, (k ^ p) * 2 + g) for g in range(2) for p in range(2)]
        pieces.append(lax.ppermute(down, ("gr", "xh"), pairs))
    blocks = jnp.stack(pieces, axis=1)
    return place_cols(gr.reshape(1), exchange(blocks, ("xl", "c")))


def body(prompt, expert_ids, route_weights, gate_master, up_master, down_master, ffn_gain):
    gr, zl = lax.axis_index("gr"), lax.axis_index("zl")
    expert = lax.axis_index(TP).reshape(1)
    ids, weights = expert_ids.T, route_weights.T
    gain = ffn_gain[:, None]
    width = prompt.shape[1]

    own_rows = dispatch(expert, ids, prompt)
    depth = lax.axis_size("zl")
    routed = [own_rows] + [shifted(own_rows, s) for s in range(1, depth)]
    down_serving = down_to_servers(down_master.astype(jnp.bfloat16), gr)
    blocks = cut(gate_master, up_master, gain)
    by_core = exchange(blocks, "c")
    own, other = by_half(by_core[:, 0], zl)
    own, other, up_blocks, routed = lax.optimization_barrier(
        (own, other, by_core[:, 1], jnp.stack(routed))
    )
    gate = to_servers(own, other, zl, gr)
    up = to_servers(*by_half(up_blocks, zl), zl, gr)
    gate_serving = gate.reshape(-1, gate.shape[-1])
    up_serving = up.reshape(-1, up.shape[-1])

    rows = lax.all_gather(routed, "y", axis=0, tiled=True).reshape(-1, width)
    gate_part = jnp.dot(rows, gate_serving, preferred_element_type=jnp.float32)
    up_part = jnp.dot(rows, up_serving, preferred_element_type=jnp.float32)
    hidden = (jax.nn.silu(gate_part) * up_part).astype(jnp.bfloat16)
    near = jnp.dot(
        hidden, down_serving[:, :NEAR], preferred_element_type=jnp.float32
    ).astype(jnp.bfloat16)
    near = lax.psum_scatter(
        near.reshape(-1, SLOTS, NEAR), "y", scatter_dimension=0, tiled=True
    )
    by_step = hidden.reshape(-1, depth, SLOTS, hidden.shape[1])
    far = [
        jnp.dot(
            by_step[:, s].reshape(-1, hidden.shape[1]),
            down_serving[:, NEAR:],
            preferred_element_type=jnp.float32,
        ).astype(jnp.bfloat16)
        for s in range(depth)
    ]
    far = [far[0]] + [shifted(far[s], -s) for s in range(1, depth)]
    far = summed(far).astype(jnp.bfloat16).reshape(-1, SLOTS, width - NEAR)
    far = exchange(far, "y")
    near = [near[0]] + [shifted(near[s], -s) for s in range(1, depth)]
    terms = combine(expert, ids, weights, near, far)
    arrived = exchange(terms.reshape(lax.axis_size(TP), -1, width), TP)
    mixed = jnp.sum(arrived.astype(jnp.float32), axis=0).astype(jnp.bfloat16)
    return (gate_serving[None], up_serving[None], down_serving[None], mixed)


def solution(mesh):
    split = Mesh(
        mesh.devices.reshape(2, 4, 8, 2, 2, 2), ("gr", "zl", "y", "xh", "xl", "c")
    )
    placed = (
        P(("gr", *FS), None),
        P(("gr", *FS), None),
        P(("gr", *FS), None),
        P("gr", FS, TP),
        P("gr", FS, TP),
        P("gr", FS, TP),
        P(FS),
    )
    return jax.shard_map(
        body,
        mesh=split,
        in_specs=placed,
        out_specs=(P(TP, None, FS), P(TP, None, FS), P(TP, FS, None), P(("gr", *FS, *TP), None)),
        check_vma=False,
    )
```

```python
import jax
import jax.numpy as jnp
from jax import lax
from jax.experimental import pallas as pl
from jax.experimental.pallas import tpu as pltpu
from jax.sharding import Mesh
from jax.sharding import PartitionSpec as P


SLOTS = 32
NEAR = 1408
NORM_EPS = 1e-06
FS = ("zl", "y")
TP = ("xh", "xl", "c")


def cut_kernel(gain_ref, gate_ref, up_ref, out_ref):
    rows, width = out_ref.shape[-2:]
    diagonal = lax.broadcasted_iota(jnp.int32, (rows, rows), 0) == lax.broadcasted_iota(
        jnp.int32, (rows, rows), 1
    )
    gain = jnp.sum(jnp.where(diagonal, gain_ref[...], 0.0), axis=1, keepdims=True)
    for i, w_ref in enumerate((gate_ref, up_ref)):
        for j in range(out_ref.shape[1]):
            cols = w_ref[0, :, j * width : (j + 1) * width]
            out_ref[0, j, 0, i] = (cols * gain).astype(jnp.bfloat16)


def cut(gate, up, gain):
    _, rows, width = gate.shape
    cols = width // 4
    weights = pl.BlockSpec((1, rows, width), lambda e: (e, 0, 0))
    return pl.pallas_call(
        cut_kernel,
        grid=(4,),
        in_specs=[pl.BlockSpec((1, rows), lambda e: (0, 0)), weights, weights],
        out_specs=pl.BlockSpec((1, 4, 1, 2, rows, cols), lambda e: (e % 2, 0, e // 2, 0, 0, 0)),
        out_shape=jax.ShapeDtypeStruct((2, 4, 2, 2, rows, cols), jnp.bfloat16),
        name="cut",
    )(gain, gate, up)


def slots_of(ids, expert):
    tokens = ids.shape[1]
    chosen = (ids[0:1] == expert) | (ids[1:2] == expert)
    before = lax.broadcasted_iota(jnp.int32, (tokens, tokens), 0) < lax.broadcasted_iota(
        jnp.int32, (tokens, tokens), 1
    )
    place = jnp.dot(
        chosen.astype(jnp.float32), before.astype(jnp.float32), preferred_element_type=jnp.float32
    ).astype(jnp.int32)
    slot = lax.broadcasted_iota(jnp.int32, (SLOTS, tokens), 0)
    return (place == slot) & chosen


def dispatch_kernel(expert_ref, ids_ref, prompt_ref, out_ref):
    x = prompt_ref[...].astype(jnp.float32)
    scale = lax.rsqrt(jnp.mean(x * x, axis=1, keepdims=True) + NORM_EPS)
    normed = (x * scale).astype(jnp.bfloat16)
    pick = slots_of(ids_ref[...], expert_ref[0]).astype(jnp.bfloat16)
    out_ref[...] = jnp.dot(pick, normed, preferred_element_type=jnp.float32).astype(jnp.bfloat16)


def dispatch(expert, ids, prompt):
    return pl.pallas_call(
        dispatch_kernel,
        in_specs=[
            pl.BlockSpec(memory_space=pltpu.SMEM),
            pl.BlockSpec(memory_space=pltpu.VMEM),
            pl.BlockSpec(memory_space=pltpu.VMEM),
        ],
        out_specs=pl.BlockSpec(memory_space=pltpu.VMEM),
        out_shape=jax.ShapeDtypeStruct((SLOTS, prompt.shape[1]), jnp.bfloat16),
        name="dispatch",
    )(expert, ids, prompt)


def summed(parts):
    total = parts[0].astype(jnp.float32)
    for i in range(1, parts.shape[0]):
        total = total + parts[i].astype(jnp.float32)
    return total


def combine_kernel(expert_ref, ids_ref, weights_ref, parts_ref, out_ref):
    pick = slots_of(ids_ref[...], expert_ref[0])
    w = jnp.where(ids_ref[0:1] == expert_ref[0], weights_ref[0:1], weights_ref[1:2])
    slot_weight = jnp.sum(jnp.where(pick, w, 0.0), axis=1, keepdims=True)
    out_ref[...] = lax.dot_general(
        pick.astype(jnp.bfloat16),
        (summed(parts_ref) * slot_weight).astype(jnp.bfloat16),
        (((0,), (0,)), ((), ())),
        preferred_element_type=jnp.float32,
    ).astype(jnp.bfloat16)


def combine(expert, ids, weights, parts):
    vmem = pl.BlockSpec(memory_space=pltpu.VMEM)
    return pl.pallas_call(
        combine_kernel,
        in_specs=[pl.BlockSpec(memory_space=pltpu.SMEM), vmem, vmem, vmem],
        out_specs=vmem,
        out_shape=jax.ShapeDtypeStruct((ids.shape[1], parts.shape[2]), jnp.bfloat16),
        name="combine",
    )(expert, ids, weights, parts)


def place_kernel(at_ref, *refs):
    *pieces, gate_ref, up_ref = refs
    rows = gate_ref.shape[2]
    for k, piece in enumerate(pieces):
        gate_ref[k ^ at_ref[0]] = piece[:, :rows]
        up_ref[k ^ at_ref[0]] = piece[:, rows:]


def place(at, pieces):
    vmem = pl.BlockSpec(memory_space=pltpu.VMEM)
    ys, rows, cols = pieces[0].shape
    out = jax.ShapeDtypeStruct((len(pieces), ys, rows // 2, cols), jnp.bfloat16)
    return pl.pallas_call(
        place_kernel,
        in_specs=[pl.BlockSpec(memory_space=pltpu.SMEM)] + [vmem] * len(pieces),
        out_specs=[vmem, vmem],
        out_shape=[out, out],
        name="place",
    )(at, *pieces)


def place_cols_kernel(at_ref, blocks_ref, out_ref):
    out_ref[...] = blocks_ref[0, 0]


def place_cols(at, blocks):
    parts, pieces, rows, width = blocks.shape
    return pl.pallas_call(
        place_cols_kernel,
        grid_spec=pltpu.PrefetchScalarGridSpec(
            num_scalar_prefetch=1,
            grid=(pieces, parts),
            in_specs=[pl.BlockSpec((1, 1, rows, width), lambda k, i, at: (i, k, 0, 0))],
            out_specs=pl.BlockSpec((rows, width), lambda k, i, at: (0, (k ^ at[0]) * parts + i)),
        ),
        out_shape=jax.ShapeDtypeStruct((rows, pieces * parts * width), jnp.bfloat16),
        name="place_cols",
    )(at, blocks)


def exchange(value, axes):
    return lax.all_to_all(value, axes, split_axis=0, concat_axis=0, tiled=True)


def rows_of_line(rows, zl):
    count = lax.axis_size("zl")
    behind = [rows]
    for step in range(1, count):
        pairs = [(z, (z - step) % count) for z in range(count)]
        behind.append(lax.ppermute(rows, "zl", pairs))
    twice = jnp.stack(behind + behind)
    return lax.dynamic_slice_in_dim(twice, (count - zl) % count, count, 0)


def by_half(by_core, zl):
    rows, cols = by_core.shape[-2:]
    by_y = exchange(by_core.reshape(16, rows, cols), ("y", "xl"))
    by_y = by_y.reshape(8, 2, rows, cols)
    own = lax.dynamic_index_in_dim(by_y, zl & 1, 1, keepdims=False)
    other = lax.dynamic_index_in_dim(by_y, 1 - (zl & 1), 1, keepdims=False)
    return own, other


def to_servers(own, other, zl, gr):
    pieces = []
    for k in range(4):
        pairs = []
        for g in range(2):
            for a in range(4):
                for p in range(2):
                    r, low = (k ^ a) >> 1, (k ^ a) & 1
                    pairs.append((g * 8 + a * 2 + p, r * 8 + (2 * p + low) * 2 + g))
        pieces.append(lax.ppermute(other if k & 1 else own, ("gr", "zl", "xh"), pairs))
    return place((2 * gr + (zl & 1)).reshape(1), pieces)


def down_to_servers(down, gr):
    pieces = []
    for k in range(2):
        pairs = [(g * 2 + p, (k ^ p) * 2 + g) for g in range(2) for p in range(2)]
        pieces.append(lax.ppermute(down, ("gr", "xh"), pairs))
    blocks = jnp.stack(pieces, axis=1)
    blocks = exchange(blocks, ("xl", "c"))
    return place_cols(gr.reshape(1), blocks)


def body(prompt, expert_ids, route_weights, gate_master, up_master, down_master, ffn_gain):
    gr, zl = lax.axis_index("gr"), lax.axis_index("zl")
    depth, servers = lax.axis_size("zl"), lax.axis_size(TP)
    expert = lax.axis_index(TP).reshape(1)
    ids, weights = expert_ids.T, route_weights.T
    width = prompt.shape[1]

    down_serving = down_to_servers(down_master.astype(jnp.bfloat16), gr)
    blocks = cut(gate_master, up_master, ffn_gain[None, :])
    by_core = exchange(blocks.reshape(2, 4, 2, -1, blocks.shape[-1]), "c")
    own_rows = dispatch(expert, ids, prompt)
    own, other = by_half(by_core, zl)
    own, other, rows = lax.optimization_barrier((own, other, rows_of_line(own_rows, zl)))
    gate, up = to_servers(own, other, zl, gr)
    gate_serving = gate.reshape(-1, gate.shape[-1])
    up_serving = up.reshape(-1, up.shape[-1])

    rows = lax.all_gather(rows, "y", axis=0, tiled=True).reshape(-1, width)
    gate_part = jnp.dot(rows, gate_serving, preferred_element_type=jnp.float32)
    up_part = jnp.dot(rows, up_serving, preferred_element_type=jnp.float32)
    hidden = (jax.nn.silu(gate_part) * up_part).astype(jnp.bfloat16)
    near = jnp.dot(hidden, down_serving[:, :NEAR], preferred_element_type=jnp.float32)
    near = near.astype(jnp.bfloat16).reshape(-1, SLOTS, NEAR)
    near = lax.psum_scatter(near, "y", scatter_dimension=0, tiled=True)
    by_depth = hidden.reshape(-1, depth, SLOTS, hidden.shape[1]).transpose(1, 0, 2, 3)
    by_depth = by_depth.reshape(hidden.shape)
    far = jnp.dot(by_depth, down_serving[:, NEAR:], preferred_element_type=jnp.float32)
    far = exchange(far.astype(jnp.bfloat16).reshape(depth, -1, width - NEAR), "zl")
    far = summed(far).astype(jnp.bfloat16).reshape(-1, SLOTS, width - NEAR)
    far = exchange(far, "y")
    far = combine(expert, ids, weights, far)
    far = exchange(far.reshape(servers, -1, width - NEAR), TP)
    near = combine(expert, ids, weights, exchange(near, "zl"))
    near = exchange(near.reshape(servers, -1, NEAR), TP)
    mixed = jnp.concatenate([summed(near), summed(far)], axis=1).astype(jnp.bfloat16)
    return (gate_serving[None], up_serving[None], down_serving[None], mixed)


def solution(mesh):
    split = Mesh(
        mesh.devices.reshape(2, 4, 8, 2, 2, 2), ("gr", "zl", "y", "xh", "xl", "c")
    )
    placed = (
        P(("gr", *FS), None),
        P(("gr", *FS), None),
        P(("gr", *FS), None),
        P("gr", FS, TP),
        P("gr", FS, TP),
        P("gr", FS, TP),
        P(FS),
    )
    return jax.shard_map(
        body,
        mesh=split,
        in_specs=placed,
        out_specs=(P(TP, None, FS), P(TP, None, FS), P(TP, FS, None), P(("gr", *FS, *TP), None)),
        check_vma=False,
    )
```

```python
import itertools

import jax
import jax.numpy as jnp
from jax import lax
from jax.experimental import pallas as pl
from jax.experimental.pallas import tpu as pltpu
from jax.sharding import Mesh
from jax.sharding import PartitionSpec as P


SLOTS = 32
NEAR = 1664
NORM_EPS = 1e-06
FS = ("zl", "y")
TP = ("xh", "xl", "c")


def cut_kernel(gain_ref, gate_ref, up_ref, out_ref):
    rows, width = out_ref.shape[-2:]
    diagonal = lax.broadcasted_iota(jnp.int32, (rows, rows), 0) == lax.broadcasted_iota(
        jnp.int32, (rows, rows), 1
    )
    gain = jnp.sum(jnp.where(diagonal, gain_ref[...], 0.0), axis=1, keepdims=True)
    for i, w_ref in enumerate((gate_ref, up_ref)):
        for j in range(out_ref.shape[1]):
            cols = w_ref[0, :, j * width : (j + 1) * width]
            out_ref[0, j, 0, i] = (cols * gain).astype(jnp.bfloat16)


def cut(gate, up, gain):
    _, rows, width = gate.shape
    cols = width // 4
    weights = pl.BlockSpec((1, rows, width), lambda e: (e, 0, 0))
    return pl.pallas_call(
        cut_kernel,
        grid=(4,),
        in_specs=[pl.BlockSpec((1, rows), lambda e: (0, 0)), weights, weights],
        out_specs=pl.BlockSpec((1, 4, 1, 2, rows, cols), lambda e: (e % 2, 0, e // 2, 0, 0, 0)),
        out_shape=jax.ShapeDtypeStruct((2, 4, 2, 2, rows, cols), jnp.bfloat16),
        name="cut",
    )(gain, gate, up)


def slots_of(ids, expert):
    tokens = ids.shape[1]
    chosen = (ids[0:1] == expert) | (ids[1:2] == expert)
    before = lax.broadcasted_iota(jnp.int32, (tokens, tokens), 0) < lax.broadcasted_iota(
        jnp.int32, (tokens, tokens), 1
    )
    place = jnp.dot(
        chosen.astype(jnp.float32), before.astype(jnp.float32), preferred_element_type=jnp.float32
    ).astype(jnp.int32)
    slot = lax.broadcasted_iota(jnp.int32, (SLOTS, tokens), 0)
    return (place == slot) & chosen


def dispatch_kernel(expert_ref, ids_ref, prompt_ref, out_ref):
    x = prompt_ref[...].astype(jnp.float32)
    scale = lax.rsqrt(jnp.mean(x * x, axis=1, keepdims=True) + NORM_EPS)
    normed = (x * scale).astype(jnp.bfloat16)
    pick = slots_of(ids_ref[...], expert_ref[0]).astype(jnp.bfloat16)
    out_ref[...] = jnp.dot(pick, normed, preferred_element_type=jnp.float32).astype(jnp.bfloat16)


def dispatch(expert, ids, prompt):
    return pl.pallas_call(
        dispatch_kernel,
        in_specs=[
            pl.BlockSpec(memory_space=pltpu.SMEM),
            pl.BlockSpec(memory_space=pltpu.VMEM),
            pl.BlockSpec(memory_space=pltpu.VMEM),
        ],
        out_specs=pl.BlockSpec(memory_space=pltpu.VMEM),
        out_shape=jax.ShapeDtypeStruct((SLOTS, prompt.shape[1]), jnp.bfloat16),
        name="dispatch",
    )(expert, ids, prompt)


def summed(parts):
    total = parts[0].astype(jnp.float32)
    for i in range(1, parts.shape[0]):
        total = total + parts[i].astype(jnp.float32)
    return total


def combine_kernel(expert_ref, ids_ref, weights_ref, parts_ref, out_ref):
    pick = slots_of(ids_ref[...], expert_ref[0])
    w = jnp.where(ids_ref[0:1] == expert_ref[0], weights_ref[0:1], weights_ref[1:2])
    slot_weight = jnp.sum(jnp.where(pick, w, 0.0), axis=1, keepdims=True)
    out_ref[...] = lax.dot_general(
        pick.astype(jnp.bfloat16),
        (summed(parts_ref) * slot_weight).astype(jnp.bfloat16),
        (((0,), (0,)), ((), ())),
        preferred_element_type=jnp.float32,
    ).astype(jnp.bfloat16)


def combine(expert, ids, weights, parts):
    vmem = pl.BlockSpec(memory_space=pltpu.VMEM)
    return pl.pallas_call(
        combine_kernel,
        in_specs=[pl.BlockSpec(memory_space=pltpu.SMEM), vmem, vmem, vmem],
        out_specs=vmem,
        out_shape=jax.ShapeDtypeStruct((ids.shape[1], parts.shape[2]), jnp.bfloat16),
        name="combine",
    )(expert, ids, weights, parts)


def place_kernel(at_ref, *refs):
    *pieces, gate_ref, up_ref = refs
    rows = gate_ref.shape[2]
    for k, piece in enumerate(pieces):
        gate_ref[k ^ at_ref[0]] = piece[:, :rows]
        up_ref[k ^ at_ref[0]] = piece[:, rows:]


def place(at, pieces):
    vmem = pl.BlockSpec(memory_space=pltpu.VMEM)
    ys, rows, cols = pieces[0].shape
    out = jax.ShapeDtypeStruct((len(pieces), ys, rows // 2, cols), jnp.bfloat16)
    return pl.pallas_call(
        place_kernel,
        in_specs=[pl.BlockSpec(memory_space=pltpu.SMEM)] + [vmem] * len(pieces),
        out_specs=[vmem, vmem],
        out_shape=[out, out],
        name="place",
    )(at, *pieces)


def place_cols_kernel(at_ref, blocks_ref, out_ref):
    out_ref[...] = blocks_ref[0, 0]


def place_cols(at, blocks):
    parts, pieces, rows, width = blocks.shape
    return pl.pallas_call(
        place_cols_kernel,
        grid_spec=pltpu.PrefetchScalarGridSpec(
            num_scalar_prefetch=1,
            grid=(pieces, parts),
            in_specs=[pl.BlockSpec((1, 1, rows, width), lambda k, i, at: (i, k, 0, 0))],
            out_specs=pl.BlockSpec((rows, width), lambda k, i, at: (0, (k ^ at[0]) * parts + i)),
        ),
        out_shape=jax.ShapeDtypeStruct((rows, pieces * parts * width), jnp.bfloat16),
        name="place_cols",
    )(at, blocks)


def exchange(value, axes):
    return lax.all_to_all(value, axes, split_axis=0, concat_axis=0, tiled=True)


def rows_of_line(rows, zl):
    count = lax.axis_size("zl")
    behind = [rows]
    for step in range(1, count):
        pairs = [(z, (z - step) % count) for z in range(count)]
        behind.append(lax.ppermute(rows, "zl", pairs))
    twice = jnp.stack(behind + behind)
    return lax.dynamic_slice_in_dim(twice, (count - zl) % count, count, 0)


def by_half(by_core, zl):
    rows, cols = by_core.shape[-2:]
    by_y = exchange(by_core.reshape(16, rows, cols), ("y", "xh"))
    by_y = by_y.reshape(8, 2, rows, cols)
    own = lax.dynamic_index_in_dim(by_y, zl & 1, 1, keepdims=False)
    other = lax.dynamic_index_in_dim(by_y, 1 - (zl & 1), 1, keepdims=False)
    return own, other


def to_servers(own, other, zl, gr):
    pieces = []
    for k in range(4):
        pairs = []
        for g, a, e, p in itertools.product(range(2), range(4), range(2), range(2)):
            r, high = (k ^ a) >> 1, (k ^ a) & 1
            pairs.append((((g * 4 + a) * 2 + e) * 2 + p, ((r * 4 + 2 * high + p) * 2 + g) * 2 + e))
        piece = other if k & 1 else own
        pieces.append(lax.ppermute(piece, ("gr", "zl", "xh", "xl"), pairs))
    return place((2 * gr + (zl >> 1)).reshape(1), pieces)


def down_to_servers(down, gr):
    pieces = []
    for k in range(2):
        pairs = [(g * 2 + p, (k ^ p) * 2 + g) for g in range(2) for p in range(2)]
        pieces.append(lax.ppermute(down, ("gr", "xh"), pairs))
    blocks = jnp.stack(pieces, axis=1)
    blocks = exchange(blocks, ("xl", "c"))
    return place_cols(gr.reshape(1), blocks)


def body(prompt, expert_ids, route_weights, gate_master, up_master, down_master, ffn_gain):
    gr, zl = lax.axis_index("gr"), lax.axis_index("zl")
    depth, servers = lax.axis_size("zl"), lax.axis_size(TP)
    expert = lax.axis_index(TP).reshape(1)
    ids, weights = expert_ids.T, route_weights.T
    width = prompt.shape[1]

    down_serving = down_to_servers(down_master.astype(jnp.bfloat16), gr)
    blocks = cut(gate_master, up_master, ffn_gain[None, :])
    by_core = exchange(blocks.reshape(2, 4, 2, -1, blocks.shape[-1]), "c")
    own_rows = dispatch(expert, ids, prompt)
    own, other = by_half(by_core, zl)
    own, other, rows = lax.optimization_barrier((own, other, rows_of_line(own_rows, zl)))
    gate, up = to_servers(own, other, zl, gr)
    gate_serving = gate.reshape(-1, gate.shape[-1])
    up_serving = up.reshape(-1, up.shape[-1])

    rows = lax.all_gather(rows, "y", axis=0, tiled=True).reshape(-1, width)
    gate_part = jnp.dot(rows, gate_serving, preferred_element_type=jnp.float32)
    up_part = jnp.dot(rows, up_serving, preferred_element_type=jnp.float32)
    hidden = (jax.nn.silu(gate_part) * up_part).astype(jnp.bfloat16)
    near = jnp.dot(hidden, down_serving[:, :NEAR], preferred_element_type=jnp.float32)
    near = near.astype(jnp.bfloat16).reshape(-1, SLOTS, NEAR)
    near = lax.psum_scatter(near, "y", scatter_dimension=0, tiled=True)
    by_depth = hidden.reshape(-1, depth, SLOTS, hidden.shape[1]).transpose(1, 0, 2, 3)
    by_depth = by_depth.reshape(hidden.shape)
    far = jnp.dot(by_depth, down_serving[:, NEAR:], preferred_element_type=jnp.float32)
    far = exchange(far.astype(jnp.bfloat16).reshape(depth, -1, width - NEAR), "zl")
    far = summed(far).astype(jnp.bfloat16).reshape(-1, SLOTS, width - NEAR)
    far = exchange(far, "y")
    far = combine(expert, ids, weights, far)
    far = exchange(far.reshape(servers, -1, width - NEAR), TP)
    near = combine(expert, ids, weights, exchange(near, "zl"))
    near = exchange(near.reshape(servers, -1, NEAR), TP)
    mixed = jnp.concatenate([summed(near), summed(far)], axis=1).astype(jnp.bfloat16)
    return (gate_serving[None], up_serving[None], down_serving[None], mixed)


def solution(mesh):
    split = Mesh(
        mesh.devices.reshape(2, 4, 8, 2, 2, 2), ("gr", "zl", "y", "xh", "xl", "c")
    )
    placed = (
        P(("gr", *FS), None),
        P(("gr", *FS), None),
        P(("gr", *FS), None),
        P("gr", FS, TP),
        P("gr", FS, TP),
        P("gr", FS, TP),
        P(FS),
    )
    return jax.shard_map(
        body,
        mesh=split,
        in_specs=placed,
        out_specs=(P(TP, None, FS), P(TP, None, FS), P(TP, FS, None), P(("gr", *FS, *TP), None)),
        check_vma=False,
    )
```

```python
import itertools

import jax
import jax.numpy as jnp
from jax import lax
from jax.experimental import pallas as pl
from jax.experimental.pallas import tpu as pltpu
from jax.sharding import Mesh
from jax.sharding import PartitionSpec as P


SLOTS = 32
NEAR = 1536
NORM_EPS = 1e-06
FS = ("zl", "y")
STEPS = (((4, -1), (0, 3), (2, -3), (-2, 1)), ((4, 1), (0, -3), (-2, 3), (2, -1)))
TP = ("xh", "xl", "c")


def cut_kernel(gain_ref, gate_ref, up_ref, out_ref):
    rows, width = out_ref.shape[-2:]
    diagonal = lax.broadcasted_iota(jnp.int32, (rows, rows), 0) == lax.broadcasted_iota(
        jnp.int32, (rows, rows), 1
    )
    gain = jnp.sum(jnp.where(diagonal, gain_ref[...], 0.0), axis=1, keepdims=True)
    for i, w_ref in enumerate((gate_ref, up_ref)):
        for j in range(out_ref.shape[1]):
            cols = w_ref[0, :, j * width : (j + 1) * width]
            out_ref[0, j, 0, i] = (cols * gain).astype(jnp.bfloat16)


def cut(gate, up, gain):
    _, rows, width = gate.shape
    cols = width // 4
    weights = pl.BlockSpec((1, rows, width), lambda e: (e, 0, 0))
    return pl.pallas_call(
        cut_kernel,
        grid=(4,),
        in_specs=[pl.BlockSpec((1, rows), lambda e: (0, 0)), weights, weights],
        out_specs=pl.BlockSpec((1, 4, 1, 2, rows, cols), lambda e: (e % 2, 0, e // 2, 0, 0, 0)),
        out_shape=jax.ShapeDtypeStruct((2, 4, 2, 2, rows, cols), jnp.bfloat16),
        name="cut",
    )(gain, gate, up)


def slots_of(ids, expert):
    tokens = ids.shape[1]
    chosen = (ids[0:1] == expert) | (ids[1:2] == expert)
    before = lax.broadcasted_iota(jnp.int32, (tokens, tokens), 0) < lax.broadcasted_iota(
        jnp.int32, (tokens, tokens), 1
    )
    place = jnp.dot(
        chosen.astype(jnp.float32), before.astype(jnp.float32), preferred_element_type=jnp.float32
    ).astype(jnp.int32)
    slot = lax.broadcasted_iota(jnp.int32, (SLOTS, tokens), 0)
    return (place == slot) & chosen


def dispatch_kernel(expert_ref, ids_ref, prompt_ref, out_ref):
    x = prompt_ref[...].astype(jnp.float32)
    scale = lax.rsqrt(jnp.mean(x * x, axis=1, keepdims=True) + NORM_EPS)
    normed = (x * scale).astype(jnp.bfloat16)
    pick = slots_of(ids_ref[...], expert_ref[0]).astype(jnp.bfloat16)
    out_ref[...] = jnp.dot(pick, normed, preferred_element_type=jnp.float32).astype(jnp.bfloat16)


def dispatch(expert, ids, prompt):
    return pl.pallas_call(
        dispatch_kernel,
        in_specs=[
            pl.BlockSpec(memory_space=pltpu.SMEM),
            pl.BlockSpec(memory_space=pltpu.VMEM),
            pl.BlockSpec(memory_space=pltpu.VMEM),
        ],
        out_specs=pl.BlockSpec(memory_space=pltpu.VMEM),
        out_shape=jax.ShapeDtypeStruct((SLOTS, prompt.shape[1]), jnp.bfloat16),
        name="dispatch",
    )(expert, ids, prompt)


def summed(parts):
    total = parts[0].astype(jnp.float32)
    for i in range(1, parts.shape[0]):
        total = total + parts[i].astype(jnp.float32)
    return total


def combine_kernel(expert_ref, ids_ref, weights_ref, near_ref, far_ref, out_ref):
    pick = slots_of(ids_ref[...], expert_ref[0])
    w = jnp.where(ids_ref[0:1] == expert_ref[0], weights_ref[0:1], weights_ref[1:2])
    slot_weight = jnp.sum(jnp.where(pick, w, 0.0), axis=1, keepdims=True)
    pick = pick.astype(jnp.bfloat16)
    first = 0
    for parts_ref in (near_ref, far_ref):
        width = parts_ref.shape[2]
        out_ref[:, first : first + width] = lax.dot_general(
            pick,
            (summed(parts_ref) * slot_weight).astype(jnp.bfloat16),
            (((0,), (0,)), ((), ())),
            preferred_element_type=jnp.float32,
        ).astype(jnp.bfloat16)
        first += width


def combine(expert, ids, weights, near, far):
    vmem = pl.BlockSpec(memory_space=pltpu.VMEM)
    width = near.shape[2] + far.shape[2]
    return pl.pallas_call(
        combine_kernel,
        in_specs=[pl.BlockSpec(memory_space=pltpu.SMEM)] + [vmem] * 4,
        out_specs=vmem,
        out_shape=jax.ShapeDtypeStruct((ids.shape[1], width), jnp.bfloat16),
        name="combine",
    )(expert, ids, weights, near, far)


def place_kernel(at_ref, *refs):
    *pieces, gate_ref, up_ref = refs
    rows = gate_ref.shape[2]
    for k, piece in enumerate(pieces):
        gate_ref[at_ref[k]] = piece[:, :rows]
        up_ref[at_ref[k]] = piece[:, rows:]


def place(at, pieces):
    vmem = pl.BlockSpec(memory_space=pltpu.VMEM)
    ys, rows, cols = pieces[0].shape
    out = jax.ShapeDtypeStruct((len(pieces), ys, rows // 2, cols), jnp.bfloat16)
    return pl.pallas_call(
        place_kernel,
        in_specs=[pl.BlockSpec(memory_space=pltpu.SMEM)] + [vmem] * len(pieces),
        out_specs=[vmem, vmem],
        out_shape=[out, out],
        name="place",
    )(at, *pieces)


def place_cols_kernel(at_ref, blocks_ref, out_ref):
    out_ref[...] = blocks_ref[0, 0]


def place_cols(at, blocks):
    parts, pieces, rows, width = blocks.shape
    return pl.pallas_call(
        place_cols_kernel,
        grid_spec=pltpu.PrefetchScalarGridSpec(
            num_scalar_prefetch=1,
            grid=(pieces, parts),
            in_specs=[pl.BlockSpec((1, 1, rows, width), lambda k, i, at: (i, k, 0, 0))],
            out_specs=pl.BlockSpec((rows, width), lambda k, i, at: (0, (k ^ at[0]) * parts + i)),
        ),
        out_shape=jax.ShapeDtypeStruct((rows, pieces * parts * width), jnp.bfloat16),
        name="place_cols",
    )(at, blocks)


def exchange(value, axes):
    return lax.all_to_all(value, axes, split_axis=0, concat_axis=0, tiled=True)


def rows_of_line(rows, zl):
    count = lax.axis_size("zl")
    behind = [rows]
    for step in range(1, count):
        pairs = [(z, (z - step) % count) for z in range(count)]
        behind.append(lax.ppermute(rows, "zl", pairs))
    twice = jnp.stack(behind + behind)
    return lax.dynamic_slice_in_dim(twice, (count - zl) % count, count, 0)


def halves(by_core, gr, zl, xl):
    rows, cols = by_core.shape[-2:]
    by_y = exchange(by_core.reshape(16, rows, cols), ("y", "xh"))
    by_y = by_y.reshape(8, 2, rows, cols)
    z = 4 * gr + zl
    out = []
    for even, odd in zip(*STEPS):
        same, other = (jnp.where(xl == 0, e, o) for e, o in zip(even, odd))
        to = z + jnp.where((z & 1) == xl, same, other)
        out.append(lax.dynamic_index_in_dim(by_y, (to >> 1) & 1, 1, keepdims=False))
    return out


def to_servers(pieces, gr, zl, xh):
    arrived, at = [], []
    for k, piece in enumerate(pieces):
        pairs = []
        for z, e, p in itertools.product(range(8), range(2), range(2)):
            to = (z + STEPS[p][k][(z ^ p) & 1]) % 8
            pairs.append(((z * 2 + e) * 2 + p, (to * 2 + z // 4) * 2 + e))
        arrived.append(lax.ppermute(piece, ("gr", "zl", "xh", "xl"), pairs))
        same, other = (jnp.where((zl & 1) == 0, e, o) for e, o in zip(STEPS[0][k], STEPS[1][k]))
        z = (4 * gr + zl - same) & 7
        at.append(jnp.where((z >> 2) == xh, z, 4 * gr + zl - other) & 3)
    return place(jnp.stack(at), arrived)


def down_to_servers(down, gr):
    pieces = []
    for k in range(2):
        pairs = [(g * 2 + p, (k ^ p) * 2 + g) for g in range(2) for p in range(2)]
        pieces.append(lax.ppermute(down, ("gr", "xh"), pairs))
    blocks = jnp.stack(pieces, axis=1)
    blocks = exchange(blocks, ("xl", "c"))
    return place_cols(gr.reshape(1), blocks)


def body(prompt, expert_ids, route_weights, gate_master, up_master, down_master, ffn_gain):
    gr, zl = lax.axis_index("gr"), lax.axis_index("zl")
    depth, servers = lax.axis_size("zl"), lax.axis_size(TP)
    expert = lax.axis_index(TP).reshape(1)
    ids, weights = expert_ids.T, route_weights.T
    width = prompt.shape[1]

    down_serving = down_to_servers(down_master.astype(jnp.bfloat16), gr)
    blocks = cut(gate_master, up_master, ffn_gain[None, :])
    by_core = exchange(blocks.reshape(2, 4, 2, -1, blocks.shape[-1]), "c")
    own_rows = dispatch(expert, ids, prompt)
    pieces = halves(by_core, gr, zl, lax.axis_index("xl"))
    pieces, rows = lax.optimization_barrier((pieces, rows_of_line(own_rows, zl)))
    gate, up = to_servers(pieces, gr, zl, lax.axis_index("xh"))
    gate_serving = gate.reshape(-1, gate.shape[-1])
    up_serving = up.reshape(-1, up.shape[-1])

    rows = lax.all_gather(rows, "y", axis=0, tiled=True).reshape(-1, width)
    gate_part = jnp.dot(rows, gate_serving, preferred_element_type=jnp.float32)
    up_part = jnp.dot(rows, up_serving, preferred_element_type=jnp.float32)
    hidden = (jax.nn.silu(gate_part) * up_part).astype(jnp.bfloat16)
    near = jnp.dot(hidden, down_serving[:, :NEAR], preferred_element_type=jnp.float32)
    near = near.astype(jnp.bfloat16).reshape(-1, SLOTS, NEAR)
    near = lax.psum_scatter(near, "y", scatter_dimension=0, tiled=True)
    by_depth = hidden.reshape(-1, depth, SLOTS, hidden.shape[1]).transpose(1, 0, 2, 3)
    by_depth = by_depth.reshape(hidden.shape)
    far = jnp.dot(by_depth, down_serving[:, NEAR:], preferred_element_type=jnp.float32)
    far = exchange(far.astype(jnp.bfloat16).reshape(depth, -1, width - NEAR), "zl")
    far = summed(far).astype(jnp.bfloat16).reshape(-1, SLOTS, width - NEAR)
    far = exchange(far, "y")
    terms = combine(expert, ids, weights, exchange(near, "zl"), far)
    arrived = exchange(terms.reshape(servers, -1, width), TP)
    mixed = summed(arrived).astype(jnp.bfloat16)
    return (gate_serving[None], up_serving[None], down_serving[None], mixed)


def solution(mesh):
    split = Mesh(
        mesh.devices.reshape(2, 4, 8, 2, 2, 2), ("gr", "zl", "y", "xh", "xl", "c")
    )
    placed = (
        P(("gr", *FS), None),
        P(("gr", *FS), None),
        P(("gr", *FS), None),
        P("gr", FS, TP),
        P("gr", FS, TP),
        P("gr", FS, TP),
        P(FS),
    )
    return jax.shard_map(
        body,
        mesh=split,
        in_specs=placed,
        out_specs=(P(TP, None, FS), P(TP, None, FS), P(TP, FS, None), P(("gr", *FS, *TP), None)),
        check_vma=False,
    )
```

```python
import itertools

import jax
import jax.numpy as jnp
from jax import lax
from jax.experimental import pallas as pl
from jax.experimental.pallas import tpu as pltpu
from jax.sharding import Mesh
from jax.sharding import PartitionSpec as P


SLOTS = 32
NEAR = 1536
NORM_EPS = 1e-06
FS = ("zl", "y")
STEPS = (((4, -1), (0, 3), (2, -3), (-2, 1)), ((4, 1), (0, -3), (-2, 3), (2, -1)))
TP = ("xh", "xl", "c")


def cut_kernel(gain_ref, gate_ref, up_ref, out_ref):
    rows, width = out_ref.shape[-2:]
    diagonal = lax.broadcasted_iota(jnp.int32, (rows, rows), 0) == lax.broadcasted_iota(
        jnp.int32, (rows, rows), 1
    )
    gain = jnp.sum(jnp.where(diagonal, gain_ref[...], 0.0), axis=1, keepdims=True)
    for i, w_ref in enumerate((gate_ref, up_ref)):
        for j in range(out_ref.shape[1]):
            cols = w_ref[0, :, j * width : (j + 1) * width]
            out_ref[0, j, 0, i] = (cols * gain).astype(jnp.bfloat16)


def cut(gate, up, gain):
    _, rows, width = gate.shape
    cols = width // 4
    weights = pl.BlockSpec((1, rows, width), lambda e: (e, 0, 0))
    return pl.pallas_call(
        cut_kernel,
        grid=(4,),
        in_specs=[pl.BlockSpec((1, rows), lambda e: (0, 0)), weights, weights],
        out_specs=pl.BlockSpec((1, 4, 1, 2, rows, cols), lambda e: (e % 2, 0, e // 2, 0, 0, 0)),
        out_shape=jax.ShapeDtypeStruct((2, 4, 2, 2, rows, cols), jnp.bfloat16),
        name="cut",
    )(gain, gate, up)


def slots_of(ids, expert):
    tokens = ids.shape[1]
    chosen = (ids[0:1] == expert) | (ids[1:2] == expert)
    before = lax.broadcasted_iota(jnp.int32, (tokens, tokens), 0) < lax.broadcasted_iota(
        jnp.int32, (tokens, tokens), 1
    )
    place = jnp.dot(
        chosen.astype(jnp.float32), before.astype(jnp.float32), preferred_element_type=jnp.float32
    ).astype(jnp.int32)
    slot = lax.broadcasted_iota(jnp.int32, (SLOTS, tokens), 0)
    return (place == slot) & chosen


def dispatch_kernel(expert_ref, ids_ref, prompt_ref, out_ref):
    x = prompt_ref[...].astype(jnp.float32)
    scale = lax.rsqrt(jnp.mean(x * x, axis=1, keepdims=True) + NORM_EPS)
    normed = (x * scale).astype(jnp.bfloat16)
    pick = slots_of(ids_ref[...], expert_ref[0]).astype(jnp.bfloat16)
    out_ref[...] = jnp.dot(pick, normed, preferred_element_type=jnp.float32).astype(jnp.bfloat16)


def dispatch(expert, ids, prompt):
    return pl.pallas_call(
        dispatch_kernel,
        in_specs=[
            pl.BlockSpec(memory_space=pltpu.SMEM),
            pl.BlockSpec(memory_space=pltpu.VMEM),
            pl.BlockSpec(memory_space=pltpu.VMEM),
        ],
        out_specs=pl.BlockSpec(memory_space=pltpu.VMEM),
        out_shape=jax.ShapeDtypeStruct((SLOTS, prompt.shape[1]), jnp.bfloat16),
        name="dispatch",
    )(expert, ids, prompt)


def summed(parts):
    total = parts[0].astype(jnp.float32)
    for i in range(1, parts.shape[0]):
        total = total + parts[i].astype(jnp.float32)
    return total


def combine_kernel(expert_ref, ids_ref, weights_ref, near_ref, far_ref, out_ref):
    pick = slots_of(ids_ref[...], expert_ref[0])
    w = jnp.where(ids_ref[0:1] == expert_ref[0], weights_ref[0:1], weights_ref[1:2])
    slot_weight = jnp.sum(jnp.where(pick, w, 0.0), axis=1, keepdims=True)
    pick = pick.astype(jnp.bfloat16)
    first = 0
    for parts_ref in (near_ref, far_ref):
        width = parts_ref.shape[2]
        out_ref[:, first : first + width] = lax.dot_general(
            pick,
            (summed(parts_ref) * slot_weight).astype(jnp.bfloat16),
            (((0,), (0,)), ((), ())),
            preferred_element_type=jnp.float32,
        ).astype(jnp.bfloat16)
        first += width


def combine(expert, ids, weights, near, far):
    vmem = pl.BlockSpec(memory_space=pltpu.VMEM)
    width = near.shape[2] + far.shape[2]
    return pl.pallas_call(
        combine_kernel,
        in_specs=[pl.BlockSpec(memory_space=pltpu.SMEM)] + [vmem] * 4,
        out_specs=vmem,
        out_shape=jax.ShapeDtypeStruct((ids.shape[1], width), jnp.bfloat16),
        name="combine",
    )(expert, ids, weights, near, far)


def place_kernel(at_ref, *refs):
    *pieces, gate_ref, up_ref = refs
    rows = gate_ref.shape[2]
    for k, piece in enumerate(pieces):
        gate_ref[at_ref[k]] = piece[:, :rows]
        up_ref[at_ref[k]] = piece[:, rows:]


def place(at, pieces):
    vmem = pl.BlockSpec(memory_space=pltpu.VMEM)
    ys, rows, cols = pieces[0].shape
    out = jax.ShapeDtypeStruct((len(pieces), ys, rows // 2, cols), jnp.bfloat16)
    return pl.pallas_call(
        place_kernel,
        in_specs=[pl.BlockSpec(memory_space=pltpu.SMEM)] + [vmem] * len(pieces),
        out_specs=[vmem, vmem],
        out_shape=[out, out],
        name="place",
    )(at, *pieces)


def place_cols_kernel(at_ref, blocks_ref, out_ref):
    out_ref[...] = blocks_ref[0, 0]


def place_cols(at, blocks):
    parts, pieces, rows, width = blocks.shape
    return pl.pallas_call(
        place_cols_kernel,
        grid_spec=pltpu.PrefetchScalarGridSpec(
            num_scalar_prefetch=1,
            grid=(pieces, parts),
            in_specs=[pl.BlockSpec((1, 1, rows, width), lambda k, i, at: (i, k, 0, 0))],
            out_specs=pl.BlockSpec(
                (rows, width), lambda k, i, at: (0, (k ^ at[0]) * parts + (i ^ at[1]))
            ),
        ),
        out_shape=jax.ShapeDtypeStruct((rows, pieces * parts * width), jnp.bfloat16),
        name="place_cols",
    )(at, blocks)


def line_up_kernel(at_ref, *refs):
    *pieces, out_ref = refs
    for s, piece in enumerate(pieces):
        out_ref[(at_ref[0] + s) % len(pieces)] = piece[...]


def line_up(at, pieces):
    vmem = pl.BlockSpec(memory_space=pltpu.VMEM)
    return pl.pallas_call(
        line_up_kernel,
        in_specs=[pl.BlockSpec(memory_space=pltpu.SMEM)] + [vmem] * len(pieces),
        out_specs=vmem,
        out_shape=jax.ShapeDtypeStruct((len(pieces), *pieces[0].shape), jnp.bfloat16),
        name="line_up",
    )(at, *pieces)


def exchange(value, axes):
    return lax.all_to_all(value, axes, split_axis=0, concat_axis=0, tiled=True)


def rows_of_line(rows, zl):
    count = lax.axis_size("zl")
    behind = [rows]
    for step in range(1, count):
        pairs = [(z, (z - step) % count) for z in range(count)]
        behind.append(lax.ppermute(rows, "zl", pairs))
    return line_up(zl.reshape(1), behind)


def halves(by_core, gr, zl, xl):
    rows, cols = by_core.shape[-2:]
    by_y = exchange(by_core.reshape(16, rows, cols), ("y", "xh"))
    by_y = by_y.reshape(8, 2, rows, cols)
    z = 4 * gr + zl
    out = []
    for even, odd in zip(*STEPS):
        same, other = (jnp.where(xl == 0, e, o) for e, o in zip(even, odd))
        to = z + jnp.where((z & 1) == xl, same, other)
        out.append(lax.dynamic_index_in_dim(by_y, (to >> 1) & 1, 1, keepdims=False))
    return out


def to_servers(pieces, gr, zl, xh):
    arrived, at = [], []
    for k, piece in enumerate(pieces):
        pairs = []
        for z, e, p in itertools.product(range(8), range(2), range(2)):
            to = (z + STEPS[p][k][(z ^ p) & 1]) % 8
            pairs.append(((z * 2 + e) * 2 + p, (to * 2 + z // 4) * 2 + e))
        arrived.append(lax.ppermute(piece, ("gr", "zl", "xh", "xl"), pairs))
        same, other = (jnp.where((zl & 1) == 0, e, o) for e, o in zip(STEPS[0][k], STEPS[1][k]))
        z = (4 * gr + zl - same) & 7
        at.append(jnp.where((z >> 2) == xh, z, 4 * gr + zl - other) & 3)
    return place(jnp.stack(at), arrived)


def down_to_servers(down, gr, own):
    pieces = []
    for k in range(2):
        pairs = [(g * 2 + p, (k ^ p) * 2 + g) for g in range(2) for p in range(2)]
        pieces.append(lax.ppermute(down, ("gr", "xh"), pairs))
    blocks = []
    for s in range(4):
        block = jnp.stack([lax.dynamic_index_in_dim(p, own ^ s, 0, keepdims=False) for p in pieces])
        if s:
            block = lax.ppermute(block, ("xl", "c"), [(u, u ^ s) for u in range(4)])
        blocks.append(block)
    return place_cols(jnp.stack([gr, own]), jnp.stack(blocks))


def body(prompt, expert_ids, route_weights, gate_master, up_master, down_master, ffn_gain):
    gr, zl = lax.axis_index("gr"), lax.axis_index("zl")
    depth, servers = lax.axis_size("zl"), lax.axis_size(TP)
    expert = lax.axis_index(TP).reshape(1)
    ids, weights = expert_ids.T, route_weights.T
    width = prompt.shape[1]

    down_serving = down_to_servers(
        down_master.astype(jnp.bfloat16), gr, lax.axis_index(("xl", "c"))
    )
    blocks = cut(gate_master, up_master, ffn_gain[None, :])
    by_core = exchange(blocks.reshape(2, 4, 2, -1, blocks.shape[-1]), "c")
    own_rows = dispatch(expert, ids, prompt)
    pieces = halves(by_core, gr, zl, lax.axis_index("xl"))
    pieces, rows = lax.optimization_barrier((pieces, rows_of_line(own_rows, zl)))
    gate, up = to_servers(pieces, gr, zl, lax.axis_index("xh"))
    gate_serving = gate.reshape(-1, gate.shape[-1])
    up_serving = up.reshape(-1, up.shape[-1])

    rows = lax.all_gather(rows, "y", axis=0, tiled=True).reshape(-1, width)
    gate_part = jnp.dot(rows, gate_serving, preferred_element_type=jnp.float32)
    up_part = jnp.dot(rows, up_serving, preferred_element_type=jnp.float32)
    hidden = (jax.nn.silu(gate_part) * up_part).astype(jnp.bfloat16)
    near = jnp.dot(hidden, down_serving[:, :NEAR], preferred_element_type=jnp.float32)
    near = near.astype(jnp.bfloat16).reshape(-1, SLOTS, NEAR)
    near = lax.psum_scatter(near, "y", scatter_dimension=0, tiled=True)
    by_depth = hidden.reshape(-1, depth, SLOTS, hidden.shape[1]).transpose(1, 0, 2, 3)
    by_depth = by_depth.reshape(hidden.shape)
    far = jnp.dot(by_depth, down_serving[:, NEAR:], preferred_element_type=jnp.float32)
    far = exchange(far.astype(jnp.bfloat16).reshape(depth, -1, width - NEAR), "zl")
    far = summed(far).astype(jnp.bfloat16).reshape(-1, SLOTS, width - NEAR)
    far = exchange(far, "y")
    terms = combine(expert, ids, weights, exchange(near, "zl"), far)
    arrived = exchange(terms.reshape(servers, -1, width), TP)
    mixed = summed(arrived).astype(jnp.bfloat16)
    return (gate_serving[None], up_serving[None], down_serving[None], mixed)


def solution(mesh):
    split = Mesh(
        mesh.devices.reshape(2, 4, 8, 2, 2, 2), ("gr", "zl", "y", "xh", "xl", "c")
    )
    placed = (
        P(("gr", *FS), None),
        P(("gr", *FS), None),
        P(("gr", *FS), None),
        P("gr", FS, TP),
        P("gr", FS, TP),
        P("gr", FS, TP),
        P(FS),
    )
    return jax.shard_map(
        body,
        mesh=split,
        in_specs=placed,
        out_specs=(P(TP, None, FS), P(TP, None, FS), P(TP, FS, None), P(("gr", *FS, *TP), None)),
        check_vma=False,
    )
```

```python
import itertools

import jax
import jax.numpy as jnp
from jax import lax
from jax.experimental import pallas as pl
from jax.experimental.pallas import tpu as pltpu
from jax.sharding import Mesh
from jax.sharding import PartitionSpec as P


SLOTS = 32
NEAR = 1536
NORM_EPS = 1e-06
FS = ("zl", "y")
STEPS = (((4, -1), (0, 3), (2, -3), (-2, 1)), ((4, 1), (0, -3), (-2, 3), (2, -1)))
TP = ("xh", "xl", "c")


def cut_kernel(gain_ref, gate_ref, up_ref, out_ref):
    rows, width = out_ref.shape[-2], out_ref.shape[-1] // 2
    diagonal = lax.broadcasted_iota(jnp.int32, (rows, rows), 0) == lax.broadcasted_iota(
        jnp.int32, (rows, rows), 1
    )
    gain = jnp.sum(jnp.where(diagonal, gain_ref[...], 0.0), axis=1, keepdims=True)
    for i, w_ref in enumerate((gate_ref, up_ref)):
        for j in range(out_ref.shape[1]):
            cols = w_ref[0, :, j * width : (j + 1) * width]
            out_ref[0, j, 0, :, i * width : (i + 1) * width] = (cols * gain).astype(jnp.bfloat16)


def cut(gate, up, gain):
    _, rows, width = gate.shape
    cols = width // 2
    weights = pl.BlockSpec((1, rows, width), lambda e: (e, 0, 0))
    return pl.pallas_call(
        cut_kernel,
        grid=(4,),
        in_specs=[pl.BlockSpec((1, rows), lambda e: (0, 0)), weights, weights],
        out_specs=pl.BlockSpec((1, 4, 1, rows, cols), lambda e: (e % 2, 0, e // 2, 0, 0)),
        out_shape=jax.ShapeDtypeStruct((2, 4, 2, rows, cols), jnp.bfloat16),
        name="cut",
    )(gain, gate, up)


def slots_of(ids, expert):
    tokens = ids.shape[1]
    chosen = (ids[0:1] == expert) | (ids[1:2] == expert)
    before = lax.broadcasted_iota(jnp.int32, (tokens, tokens), 0) < lax.broadcasted_iota(
        jnp.int32, (tokens, tokens), 1
    )
    place = jnp.dot(
        chosen.astype(jnp.float32), before.astype(jnp.float32), preferred_element_type=jnp.float32
    ).astype(jnp.int32)
    slot = lax.broadcasted_iota(jnp.int32, (SLOTS, tokens), 0)
    return (place == slot) & chosen


def dispatch_kernel(expert_ref, ids_ref, prompt_ref, out_ref):
    x = prompt_ref[...].astype(jnp.float32)
    scale = lax.rsqrt(jnp.mean(x * x, axis=1, keepdims=True) + NORM_EPS)
    normed = (x * scale).astype(jnp.bfloat16)
    pick = slots_of(ids_ref[...], expert_ref[0]).astype(jnp.bfloat16)
    out_ref[...] = jnp.dot(pick, normed, preferred_element_type=jnp.float32).astype(jnp.bfloat16)


def dispatch(expert, ids, prompt):
    return pl.pallas_call(
        dispatch_kernel,
        in_specs=[
            pl.BlockSpec(memory_space=pltpu.SMEM),
            pl.BlockSpec(memory_space=pltpu.VMEM),
            pl.BlockSpec(memory_space=pltpu.VMEM),
        ],
        out_specs=pl.BlockSpec(memory_space=pltpu.VMEM),
        out_shape=jax.ShapeDtypeStruct((SLOTS, prompt.shape[1]), jnp.bfloat16),
        name="dispatch",
    )(expert, ids, prompt)


def summed(parts):
    total = parts[0].astype(jnp.float32)
    for i in range(1, parts.shape[0]):
        total = total + parts[i].astype(jnp.float32)
    return total


def combine_kernel(expert_ref, ids_ref, weights_ref, near_ref, far_ref, out_ref):
    pick = slots_of(ids_ref[...], expert_ref[0])
    w = jnp.where(ids_ref[0:1] == expert_ref[0], weights_ref[0:1], weights_ref[1:2])
    slot_weight = jnp.sum(jnp.where(pick, w, 0.0), axis=1, keepdims=True)
    pick = pick.astype(jnp.bfloat16)
    first = 0
    for parts_ref in (near_ref, far_ref):
        width = parts_ref.shape[2]
        out_ref[:, first : first + width] = lax.dot_general(
            pick,
            (summed(parts_ref) * slot_weight).astype(jnp.bfloat16),
            (((0,), (0,)), ((), ())),
            preferred_element_type=jnp.float32,
        ).astype(jnp.bfloat16)
        first += width


def combine(expert, ids, weights, near, far):
    vmem = pl.BlockSpec(memory_space=pltpu.VMEM)
    width = near.shape[2] + far.shape[2]
    return pl.pallas_call(
        combine_kernel,
        in_specs=[pl.BlockSpec(memory_space=pltpu.SMEM)] + [vmem] * 4,
        out_specs=vmem,
        out_shape=jax.ShapeDtypeStruct((ids.shape[1], width), jnp.bfloat16),
        name="combine",
    )(expert, ids, weights, near, far)


def place_kernel(at_ref, *refs):
    *pieces, gate_ref, up_ref = refs
    width = gate_ref.shape[2]
    for k, piece in enumerate(pieces):
        gate_ref[at_ref[k]] = piece[:, :width]
        up_ref[at_ref[k]] = piece[:, width:]


def place(at, pieces):
    vmem = pl.BlockSpec(memory_space=pltpu.VMEM)
    rows, cols = pieces[0].shape
    out = jax.ShapeDtypeStruct((len(pieces), rows, cols // 2), jnp.bfloat16)
    return pl.pallas_call(
        place_kernel,
        in_specs=[pl.BlockSpec(memory_space=pltpu.SMEM)] + [vmem] * len(pieces),
        out_specs=[vmem, vmem],
        out_shape=[out, out],
        name="place",
    )(at, *pieces)


def place_cols_kernel(at_ref, blocks_ref, out_ref):
    out_ref[...] = blocks_ref[0, 0]


def place_cols(at, blocks):
    parts, pieces, rows, width = blocks.shape
    return pl.pallas_call(
        place_cols_kernel,
        grid_spec=pltpu.PrefetchScalarGridSpec(
            num_scalar_prefetch=1,
            grid=(pieces, parts),
            in_specs=[pl.BlockSpec((1, 1, rows, width), lambda k, i, at: (i, k, 0, 0))],
            out_specs=pl.BlockSpec(
                (rows, width), lambda k, i, at: (0, (k ^ at[0]) * parts + (i ^ at[1]))
            ),
        ),
        out_shape=jax.ShapeDtypeStruct((rows, pieces * parts * width), jnp.bfloat16),
        name="place_cols",
    )(at, blocks)


def line_up_kernel(at_ref, *refs):
    *pieces, out_ref = refs
    for s, piece in enumerate(pieces):
        out_ref[(at_ref[0] + s) % len(pieces)] = piece[...]


def line_up(at, pieces):
    vmem = pl.BlockSpec(memory_space=pltpu.VMEM)
    return pl.pallas_call(
        line_up_kernel,
        in_specs=[pl.BlockSpec(memory_space=pltpu.SMEM)] + [vmem] * len(pieces),
        out_specs=vmem,
        out_shape=jax.ShapeDtypeStruct((len(pieces), *pieces[0].shape), jnp.bfloat16),
        name="line_up",
    )(at, *pieces)


def exchange(value, axes):
    return lax.all_to_all(value, axes, split_axis=0, concat_axis=0, tiled=True)


def rows_of_line(rows, zl):
    count = lax.axis_size("zl")
    behind = [rows]
    for step in range(1, count):
        pairs = [(z, (z - step) % count) for z in range(count)]
        behind.append(lax.ppermute(rows, "zl", pairs))
    return line_up(zl.reshape(1), behind)


def halves(by_core, gr, zl, xl):
    rows, cols = by_core.shape[-2:]
    by_y = exchange(by_core.reshape(16, rows, cols), ("y", "xh"))
    by_y = by_y.reshape(8, 2, rows, cols)
    z = 4 * gr + zl
    out = []
    for even, odd in zip(*STEPS):
        same, other = (jnp.where(xl == 0, e, o) for e, o in zip(even, odd))
        to = z + jnp.where((z & 1) == xl, same, other)
        half = lax.dynamic_index_in_dim(by_y, (to >> 1) & 1, 1, keepdims=False)
        out.append(half.reshape(8 * rows, cols))
    return out


def to_servers(pieces, gr, zl, xh):
    arrived, at = [], []
    for k, piece in enumerate(pieces):
        pairs = []
        for z, e, p in itertools.product(range(8), range(2), range(2)):
            to = (z + STEPS[p][k][(z ^ p) & 1]) % 8
            pairs.append(((z * 2 + e) * 2 + p, (to * 2 + z // 4) * 2 + e))
        arrived.append(lax.ppermute(piece, ("gr", "zl", "xh", "xl"), pairs))
        same, other = (jnp.where((zl & 1) == 0, e, o) for e, o in zip(STEPS[0][k], STEPS[1][k]))
        z = (4 * gr + zl - same) & 7
        at.append(jnp.where((z >> 2) == xh, z, 4 * gr + zl - other) & 3)
    return arrived, at


def down_to_servers(down, gr, own):
    pieces = []
    for k in range(2):
        pairs = [(g * 2 + p, (k ^ p) * 2 + g) for g in range(2) for p in range(2)]
        pieces.append(lax.ppermute(down, ("gr", "xh"), pairs))
    blocks = []
    for s in range(4):
        block = [lax.dynamic_index_in_dim(p, own ^ s, 0, keepdims=False) for p in pieces]
        block = jnp.stack(block)
        if s:
            block = lax.ppermute(block, ("xl", "c"), [(u, u ^ s) for u in range(4)])
        blocks.append(block)
    return place_cols(jnp.stack([gr, own]), jnp.stack(blocks))


def body(prompt, expert_ids, route_weights, gate_master, up_master, down_master, ffn_gain):
    gr, zl = lax.axis_index("gr"), lax.axis_index("zl")
    depth, servers = lax.axis_size("zl"), lax.axis_size(TP)
    expert = lax.axis_index(TP).reshape(1)
    ids, weights = expert_ids.T, route_weights.T
    width = prompt.shape[1]

    down_serving = down_to_servers(
        down_master.astype(jnp.bfloat16), gr, lax.axis_index(("xl", "c"))
    )
    blocks = cut(gate_master, up_master, ffn_gain[None, :])
    by_core = exchange(blocks, "c")
    own_rows = dispatch(expert, ids, prompt)
    pieces = halves(by_core, gr, zl, lax.axis_index("xl"))
    pieces, rows = lax.optimization_barrier((pieces, rows_of_line(own_rows, zl)))
    pieces, at = to_servers(pieces, gr, zl, lax.axis_index("xh"))
    gate, up = place(jnp.stack(at), pieces)
    gate_serving = gate.reshape(-1, gate.shape[-1])
    up_serving = up.reshape(-1, up.shape[-1])

    rows = lax.all_gather(rows, "y", axis=0, tiled=True).reshape(-1, width)
    both = 0.0
    for k, piece in enumerate(pieces):
        cols = lax.dynamic_slice_in_dim(rows, at[k] * piece.shape[0], piece.shape[0], 1)
        both = both + jnp.dot(cols, piece, preferred_element_type=jnp.float32)
    gate_part, up_part = jnp.split(both, 2, axis=1)
    hidden = (jax.nn.silu(gate_part) * up_part).astype(jnp.bfloat16)
    near = jnp.dot(hidden, down_serving[:, :NEAR], preferred_element_type=jnp.float32)
    near = near.astype(jnp.bfloat16).reshape(-1, SLOTS, NEAR)
    near = lax.psum_scatter(near, "y", scatter_dimension=0, tiled=True)
    by_depth = hidden.reshape(-1, depth, SLOTS, hidden.shape[1]).transpose(1, 0, 2, 3)
    by_depth = by_depth.reshape(hidden.shape)
    far = jnp.dot(by_depth, down_serving[:, NEAR:], preferred_element_type=jnp.float32)
    far = exchange(far.astype(jnp.bfloat16).reshape(depth, -1, width - NEAR), "zl")
    far = summed(far).astype(jnp.bfloat16).reshape(-1, SLOTS, width - NEAR)
    far = exchange(far, "y")
    terms = combine(expert, ids, weights, exchange(near, "zl"), far)
    arrived = exchange(terms.reshape(servers, -1, width), TP)
    mixed = summed(arrived).astype(jnp.bfloat16)
    return (gate_serving[None], up_serving[None], down_serving[None], mixed)


def solution(mesh):
    split = Mesh(
        mesh.devices.reshape(2, 4, 8, 2, 2, 2), ("gr", "zl", "y", "xh", "xl", "c")
    )
    placed = (
        P(("gr", *FS), None),
        P(("gr", *FS), None),
        P(("gr", *FS), None),
        P("gr", FS, TP),
        P("gr", FS, TP),
        P("gr", FS, TP),
        P(FS),
    )
    return jax.shard_map(
        body,
        mesh=split,
        in_specs=placed,
        out_specs=(P(TP, None, FS), P(TP, None, FS), P(TP, FS, None), P(("gr", *FS, *TP), None)),
        check_vma=False,
    )
```

```python
import itertools

import jax
import jax.numpy as jnp
from jax import lax
from jax.experimental import pallas as pl
from jax.experimental.pallas import tpu as pltpu
from jax.sharding import Mesh
from jax.sharding import PartitionSpec as P


SLOTS = 32
NEAR = 1536
NORM_EPS = 1e-06
FS = ("zl", "y")
STEPS = (((4, -1), (0, 3), (2, -3), (-2, 1)), ((4, 1), (0, -3), (-2, 3), (2, -1)))
TP = ("xh", "xl", "c")


def cut_kernel(gain_ref, gate_ref, up_ref, out_ref):
    rows, width = out_ref.shape[-2], out_ref.shape[-1] // 2
    diagonal = lax.broadcasted_iota(jnp.int32, (rows, rows), 0) == lax.broadcasted_iota(
        jnp.int32, (rows, rows), 1
    )
    gain = jnp.sum(jnp.where(diagonal, gain_ref[...], 0.0), axis=1, keepdims=True)
    for i, w_ref in enumerate((gate_ref, up_ref)):
        for j in range(out_ref.shape[1]):
            cols = w_ref[0, :, j * width : (j + 1) * width]
            out_ref[0, j, 0, :, i * width : (i + 1) * width] = (cols * gain).astype(jnp.bfloat16)


def cut(gate, up, gain):
    _, rows, width = gate.shape
    cols = width // 2
    weights = pl.BlockSpec((1, rows, width), lambda e: (e, 0, 0))
    return pl.pallas_call(
        cut_kernel,
        grid=(4,),
        in_specs=[pl.BlockSpec((1, rows), lambda e: (0, 0)), weights, weights],
        out_specs=pl.BlockSpec((1, 4, 1, rows, cols), lambda e: (e % 2, 0, e // 2, 0, 0)),
        out_shape=jax.ShapeDtypeStruct((2, 4, 2, rows, cols), jnp.bfloat16),
        name="cut",
    )(gain, gate, up)


def slots_of(ids, expert):
    tokens = ids.shape[1]
    chosen = (ids[0:1] == expert) | (ids[1:2] == expert)
    before = lax.broadcasted_iota(jnp.int32, (tokens, tokens), 0) < lax.broadcasted_iota(
        jnp.int32, (tokens, tokens), 1
    )
    place = jnp.dot(
        chosen.astype(jnp.float32), before.astype(jnp.float32), preferred_element_type=jnp.float32
    ).astype(jnp.int32)
    slot = lax.broadcasted_iota(jnp.int32, (SLOTS, tokens), 0)
    return (place == slot) & chosen


def dispatch_kernel(expert_ref, ids_ref, prompt_ref, out_ref):
    x = prompt_ref[...].astype(jnp.float32)
    scale = lax.rsqrt(jnp.mean(x * x, axis=1, keepdims=True) + NORM_EPS)
    normed = (x * scale).astype(jnp.bfloat16)
    pick = slots_of(ids_ref[...], expert_ref[0]).astype(jnp.bfloat16)
    out_ref[...] = jnp.dot(pick, normed, preferred_element_type=jnp.float32).astype(jnp.bfloat16)


def dispatch(expert, ids, prompt):
    return pl.pallas_call(
        dispatch_kernel,
        in_specs=[
            pl.BlockSpec(memory_space=pltpu.SMEM),
            pl.BlockSpec(memory_space=pltpu.VMEM),
            pl.BlockSpec(memory_space=pltpu.VMEM),
        ],
        out_specs=pl.BlockSpec(memory_space=pltpu.VMEM),
        out_shape=jax.ShapeDtypeStruct((SLOTS, prompt.shape[1]), jnp.bfloat16),
        name="dispatch",
    )(expert, ids, prompt)


def summed(parts):
    total = parts[0].astype(jnp.float32)
    for i in range(1, parts.shape[0]):
        total = total + parts[i].astype(jnp.float32)
    return total


def combine_kernel(expert_ref, ids_ref, weights_ref, near_ref, far_ref, out_ref):
    pick = slots_of(ids_ref[...], expert_ref[0])
    w = jnp.where(ids_ref[0:1] == expert_ref[0], weights_ref[0:1], weights_ref[1:2])
    slot_weight = jnp.sum(jnp.where(pick, w, 0.0), axis=1, keepdims=True)
    pick = pick.astype(jnp.bfloat16)
    first = 0
    for parts_ref in (near_ref, far_ref):
        width = parts_ref.shape[2]
        out_ref[:, first : first + width] = lax.dot_general(
            pick,
            (summed(parts_ref) * slot_weight).astype(jnp.bfloat16),
            (((0,), (0,)), ((), ())),
            preferred_element_type=jnp.float32,
        ).astype(jnp.bfloat16)
        first += width


def combine(expert, ids, weights, near, far):
    vmem = pl.BlockSpec(memory_space=pltpu.VMEM)
    width = near.shape[2] + far.shape[2]
    return pl.pallas_call(
        combine_kernel,
        in_specs=[pl.BlockSpec(memory_space=pltpu.SMEM)] + [vmem] * 4,
        out_specs=vmem,
        out_shape=jax.ShapeDtypeStruct((ids.shape[1], width), jnp.bfloat16),
        name="combine",
    )(expert, ids, weights, near, far)


def place_kernel(at_ref, *refs):
    *pieces, gate_ref, up_ref = refs
    width = gate_ref.shape[2]
    for k, piece in enumerate(pieces):
        gate_ref[at_ref[k]] = piece[:, :width]
        up_ref[at_ref[k]] = piece[:, width:]


def place(at, pieces):
    vmem = pl.BlockSpec(memory_space=pltpu.VMEM)
    rows, cols = pieces[0].shape
    out = jax.ShapeDtypeStruct((len(pieces), rows, cols // 2), jnp.bfloat16)
    return pl.pallas_call(
        place_kernel,
        in_specs=[pl.BlockSpec(memory_space=pltpu.SMEM)] + [vmem] * len(pieces),
        out_specs=[vmem, vmem],
        out_shape=[out, out],
        name="place",
    )(at, *pieces)


def place_cols_kernel(at_ref, blocks_ref, out_ref):
    out_ref[...] = blocks_ref[0, 0]


def place_cols(at, blocks):
    parts, pieces, rows, width = blocks.shape
    return pl.pallas_call(
        place_cols_kernel,
        grid_spec=pltpu.PrefetchScalarGridSpec(
            num_scalar_prefetch=1,
            grid=(pieces, parts),
            in_specs=[pl.BlockSpec((1, 1, rows, width), lambda k, i, at: (i, k, 0, 0))],
            out_specs=pl.BlockSpec(
                (rows, width), lambda k, i, at: (0, (k ^ at[0]) * parts + (i ^ at[1]))
            ),
        ),
        out_shape=jax.ShapeDtypeStruct((rows, pieces * parts * width), jnp.bfloat16),
        name="place_cols",
    )(at, blocks)


def line_up_kernel(at_ref, *refs):
    *pieces, out_ref = refs
    for s, piece in enumerate(pieces):
        out_ref[(at_ref[0] + s) % len(pieces)] = piece[...]


def line_up(at, pieces):
    vmem = pl.BlockSpec(memory_space=pltpu.VMEM)
    return pl.pallas_call(
        line_up_kernel,
        in_specs=[pl.BlockSpec(memory_space=pltpu.SMEM)] + [vmem] * len(pieces),
        out_specs=vmem,
        out_shape=jax.ShapeDtypeStruct((len(pieces), *pieces[0].shape), jnp.bfloat16),
        name="line_up",
    )(at, *pieces)


def exchange(value, axes):
    return lax.all_to_all(value, axes, split_axis=0, concat_axis=0, tiled=True)


def rows_of_line(rows, zl):
    count = lax.axis_size("zl")
    behind = [rows]
    for step in range(1, count):
        pairs = [(z, (z - step) % count) for z in range(count)]
        behind.append(lax.ppermute(rows, "zl", pairs))
    return line_up(zl.reshape(1), behind)


def halves(by_core, gr, zl, xl):
    rows, cols = by_core.shape[-2:]
    by_y = exchange(by_core.reshape(16, rows, cols), ("y", "xh"))
    by_y = by_y.reshape(8, 2, rows, cols)
    z = 4 * gr + zl
    out = []
    for even, odd in zip(*STEPS):
        same, other = (jnp.where(xl == 0, e, o) for e, o in zip(even, odd))
        to = z + jnp.where((z & 1) == xl, same, other)
        half = lax.dynamic_index_in_dim(by_y, (to >> 1) & 1, 1, keepdims=False)
        out.append(half.reshape(8 * rows, cols))
    return out


def to_servers(pieces, gr, zl, xh):
    at = []
    for even, odd in zip(*STEPS):
        same, other = (jnp.where((zl & 1) == 0, e, o) for e, o in zip(even, odd))
        z = (4 * gr + zl - same) & 7
        at.append(jnp.where((z >> 2) == xh, z, 4 * gr + zl - other) & 3)

    def send(value, k, across):
        pairs = []
        for z, e, p in itertools.product(range(8), range(2), range(2)):
            to = (z + STEPS[p][k][(z ^ p) & 1]) % 8
            pairs.append(((z * 2 + e) * 2 + (p ^ across), (to * 2 + z // 4) * 2 + e))
        return lax.ppermute(value, ("gr", "zl", "xh", "xl"), pairs)

    half = pieces[0].shape[1] // 2
    across = lax.ppermute(pieces[0][:, half:], "xl", [(0, 1), (1, 0)])
    longest = [send(pieces[0][:, :half], 0, 0), send(across, 0, 1)]
    arrived = [send(pieces[k], k, 0) for k in range(1, 4)]
    return [jnp.concatenate(longest, axis=1)] + arrived, at


def down_to_servers(down, gr, own):
    pieces = []
    for k in range(2):
        pairs = [(g * 2 + p, (k ^ p) * 2 + g) for g in range(2) for p in range(2)]
        pieces.append(lax.ppermute(down, ("gr", "xh"), pairs))
    blocks = []
    for s in range(4):
        block = [lax.dynamic_index_in_dim(p, own ^ s, 0, keepdims=False) for p in pieces]
        block = jnp.stack(block)
        if s:
            block = lax.ppermute(block, ("xl", "c"), [(u, u ^ s) for u in range(4)])
        blocks.append(block)
    at = jnp.stack([gr, own])
    blocks = jnp.stack(blocks)
    return place_cols(at, blocks)


def body(prompt, expert_ids, route_weights, gate_master, up_master, down_master, ffn_gain):
    gr, zl = lax.axis_index("gr"), lax.axis_index("zl")
    depth, servers = lax.axis_size("zl"), lax.axis_size(TP)
    expert = lax.axis_index(TP).reshape(1)
    ids, weights = expert_ids.T, route_weights.T
    width = prompt.shape[1]

    down_serving = down_to_servers(
        down_master.astype(jnp.bfloat16), gr, lax.axis_index(("xl", "c"))
    )
    blocks = cut(gate_master, up_master, ffn_gain[None, :])
    by_core = exchange(blocks, "c")
    own_rows = dispatch(expert, ids, prompt)
    pieces = halves(by_core, gr, zl, lax.axis_index("xl"))
    pieces, rows = lax.optimization_barrier((pieces, rows_of_line(own_rows, zl)))
    pieces, at = to_servers(pieces, gr, zl, lax.axis_index("xh"))
    gate, up = place(jnp.stack(at), pieces)
    gate_serving = gate.reshape(-1, gate.shape[-1])
    up_serving = up.reshape(-1, up.shape[-1])

    rows = lax.all_gather(rows, "y", axis=0, tiled=True).reshape(-1, width)
    both = 0.0
    for k in (1, 2, 3, 0):
        piece = pieces[k]
        cols = lax.dynamic_slice_in_dim(rows, at[k] * piece.shape[0], piece.shape[0], 1)
        both = both + jnp.dot(cols, piece, preferred_element_type=jnp.float32)
    gate_part, up_part = jnp.split(both, 2, axis=1)
    hidden = (jax.nn.silu(gate_part) * up_part).astype(jnp.bfloat16)
    near = jnp.dot(hidden, down_serving[:, :NEAR], preferred_element_type=jnp.float32)
    near = near.astype(jnp.bfloat16).reshape(-1, SLOTS, NEAR)
    near = lax.psum_scatter(near, "y", scatter_dimension=0, tiled=True)
    by_depth = hidden.reshape(-1, depth, SLOTS, hidden.shape[1]).transpose(1, 0, 2, 3)
    by_depth = by_depth.reshape(hidden.shape)
    far = jnp.dot(by_depth, down_serving[:, NEAR:], preferred_element_type=jnp.float32)
    far = exchange(far.astype(jnp.bfloat16).reshape(depth, -1, width - NEAR), "zl")
    far = summed(far).astype(jnp.bfloat16).reshape(-1, SLOTS, width - NEAR)
    far = exchange(far, "y")
    terms = combine(expert, ids, weights, exchange(near, "zl"), far)
    arrived = exchange(terms.reshape(servers, -1, width), TP)
    mixed = summed(arrived).astype(jnp.bfloat16)
    return (gate_serving[None], up_serving[None], down_serving[None], mixed)


def solution(mesh):
    split = Mesh(
        mesh.devices.reshape(2, 4, 8, 2, 2, 2), ("gr", "zl", "y", "xh", "xl", "c")
    )
    placed = (
        P(("gr", *FS), None),
        P(("gr", *FS), None),
        P(("gr", *FS), None),
        P("gr", FS, TP),
        P("gr", FS, TP),
        P("gr", FS, TP),
        P(FS),
    )
    return jax.shard_map(
        body,
        mesh=split,
        in_specs=placed,
        out_specs=(P(TP, None, FS), P(TP, None, FS), P(TP, FS, None), P(("gr", *FS, *TP), None)),
        check_vma=False,
    )
```
